512 devices in a mesh: sp: 64 (over z, y), fs: 4 (over x), tp: 2 (over core).
Axes of the slice: x: 4, y: 8, z: 8, core: 2. Of those that a mesh axis runs over, the one named last changes fastest.
Arguments:
- queries: bfloat16 [4, 16384, 512], P('fs', 'sp', 'tp'), may hold values from -60 to 60
- keys: bfloat16 [4, 16384, 256], P('fs', 'sp', 'tp'), may hold values from -4.5 to 4.5
- values: bfloat16 [4, 16384, 256], P('fs', 'sp', 'tp'), may hold values from -6 to 6
- forget_cache: float32 [4, 16384, 8], P('fs', 'sp', 'tp'), may hold values from -2048 to 0, as said below
- fox_gain: float32 [512], P('tp'), may hold values from 0.1 to 1.9
- receptance: bfloat16 [4, 16384, 512], P('fs', 'sp', 'tp'), may hold values from -6 to 6
- lin_keys: bfloat16 [4, 16384, 512], P('fs', 'sp', 'tp'), may hold values from -6 to 6
- lin_values: bfloat16 [4, 16384, 512], P('fs', 'sp', 'tp'), may hold values from -6 to 6
- learn_logit: bfloat16 [4, 16384, 512], P('fs', 'sp', 'tp'), may hold values from -12 to 4
- decay_log: float32 [4, 16384, 512], P('fs', 'sp', 'tp'), may hold values from -16 to 0
- lin_gain: float32 [512], P('tp'), may hold values from 0.1 to 1.9
- out_fox_weight: bfloat16 [512, 2048], P('tp', 'fs'), may hold values from -0.1875 to 0.1875
- out_lin_weight: bfloat16 [512, 2048], P('tp', 'fs'), may hold values from -0.1875 to 0.1875
Outputs:
- mixed: bfloat16 [4, 16384, 2048], P('fs', ('sp', 'tp'))
The draws below stay inside these ranges and needn't reach their ends.
Inputs may be any that keep to these rules, and one draw needn't show every extreme that they name: `forget_cache`: Non-increasing along the positions of each sequence and head.
All inputs are finite; a program needn't handle non-finite values.
Results may differ from the reference program's by a relative error of at most 0.017.
Values may be sent and summed in bfloat16 or wider, within the bound.
A program may use at most 64 MiB of HBM per device.

```python
import math
import jax
import jax.numpy as jnp
from jax import lax

D = 2048
HEAD = 64
FOX_HEADS = 8
KEY_HEADS = 4
LIN_HEADS = 8
TOK_DEV = 256
W_FOX = 512
W_LIN = 512
SEQUENCE_COUNT = 4
SEQUENCE_LENGTH = 16384
N_TP = 2


def slow_flags(key, salt, count):
    order = jax.random.permutation(jax.random.fold_in(key, salt), count)
    return order < count // 2


def lin_flags(key):
    return jnp.repeat(slow_flags(key, 5, LIN_HEADS), HEAD)


def step_rates(key, salt, count, slow_heads):
    split_keys = jax.random.split(jax.random.fold_in(key, salt), 6)
    chain_total = jax.random.uniform(split_keys[0], (SEQUENCE_COUNT, 1, count), jnp.float32, 0.15, 0.5)
    reach_steps = jax.random.uniform(split_keys[1], (SEQUENCE_COUNT, 1, count), jnp.float32, 30.0, 100.0)
    baseline_rate = jnp.where(slow_heads[None, None, :], chain_total / SEQUENCE_LENGTH, 1.0 / reach_steps)
    block_list = jnp.exp(jax.random.uniform(split_keys[2], (SEQUENCE_COUNT, SEQUENCE_LENGTH // TOK_DEV, 1), jnp.float32, -0.7, 0.7))
    block_list = jnp.repeat(block_list, TOK_DEV, axis=1)
    nearby_factor = jax.random.uniform(split_keys[3], (SEQUENCE_COUNT, SEQUENCE_LENGTH, count), jnp.float32, 0.3, 1.7)
    spurt_rows = jax.random.randint(split_keys[4], (SEQUENCE_COUNT, 3), 0, SEQUENCE_LENGTH)
    spurt_depth = jax.random.uniform(split_keys[5], (SEQUENCE_COUNT, 3), jnp.float32, 0.22, 0.5)
    matched_rows = (jnp.arange(SEQUENCE_LENGTH)[None, :, None] == spurt_rows[:, None, :]).astype(jnp.float32)
    spurt_groups = jnp.sum(matched_rows * spurt_depth[:, None, :], axis=-1)
    gradual_float = slow_heads.astype(jnp.float32)
    return baseline_rate * block_list * nearby_factor + spurt_groups[:, :, None] * gradual_float[None, None, :]


def query_key(key):
    split_keys = jax.random.split(jax.random.fold_in(key, 7), 2)
    key_float = jnp.clip(jax.random.normal(split_keys[0], (SEQUENCE_COUNT, SEQUENCE_LENGTH, KEY_HEADS * HEAD), jnp.float32), -4.5, 4.5)
    query_float = jnp.clip(1.5 * jax.random.normal(split_keys[1], (SEQUENCE_COUNT, SEQUENCE_LENGTH, FOX_HEADS * HEAD), jnp.float32), -9.0, 9.0)
    return (query_float, key_float)


def draw_queries(key, part):
    return query_key(key)[0].astype(jnp.bfloat16)


def draw_keys(key, part):
    return query_key(key)[1].astype(jnp.bfloat16)


def draw_forget_cache(key, part):
    slow_heads = slow_flags(key, 3, FOX_HEADS)
    rates = step_rates(key, 13, FOX_HEADS, slow_heads)
    return -jnp.cumsum(rates, axis=1)


def draw_decay_log(key, part):
    slow_heads = lin_flags(key)
    return jnp.log(step_rates(key, 17, LIN_HEADS * HEAD, slow_heads))


def draw_learn_logit(key, part):
    slow_heads = lin_flags(key)
    noise_key = jax.random.fold_in(key, 23)
    spread = jnp.clip(jax.random.normal(noise_key, (SEQUENCE_COUNT, SEQUENCE_LENGTH, LIN_HEADS * HEAD), jnp.float32), -4.0, 4.0)
    return (spread - 8.0 * slow_heads.astype(jnp.float32)[None, None, :]).astype(jnp.bfloat16)


def shard_levels(key, shape, cuts, least, high):
    loudness = 1.0
    for position, parts in cuts:
        steps = jax.random.uniform(jax.random.fold_in(jax.random.fold_in(key, 6), position), (parts,), jnp.float32, least / len(cuts), high / len(cuts))
        loudness = loudness * jnp.repeat(jnp.exp(steps), shape[position] // parts).reshape((-1,) + (1,) * (len(shape) - 1 - position))
    return loudness


def bell_draw(key, shape, scale, bound, cuts=(), held_as=jnp.bfloat16):
    drawn = jax.random.normal(key, shape, jnp.float32) * scale
    if len(cuts) > 0:
        drawn = shard_levels(key, shape, cuts, -0.22, 0.18) * drawn
    return jnp.clip(drawn, min=-bound, max=bound).astype(held_as)


def setup_inputs(seed: int = 0) -> dict:
    key_of = jax.random.split(jax.random.key(seed), 14)
    return {
        "queries": draw_queries(jax.random.fold_in(key_of[13], 71), 0),
        "keys": draw_keys(jax.random.fold_in(key_of[13], 71), 0),
        "values": bell_draw(key_of[2], (SEQUENCE_COUNT, SEQUENCE_LENGTH, KEY_HEADS * HEAD), 1.0, 6.0, ((0, 4), (1, 64), (2, 2))),
        "forget_cache": draw_forget_cache(jax.random.fold_in(key_of[13], 71), 0),
        "fox_gain": jnp.clip(1.0 + 0.18 * jax.random.normal(key_of[4], (W_FOX,), jnp.float32), 0.1, 1.9),
        "receptance": bell_draw(key_of[5], (SEQUENCE_COUNT, SEQUENCE_LENGTH, W_LIN), 1.0, 6.0, ((0, 4), (1, 64), (2, 2))),
        "lin_keys": bell_draw(key_of[6], (SEQUENCE_COUNT, SEQUENCE_LENGTH, W_LIN), 1.0, 6.0, ((0, 4), (1, 64), (2, 2))),
        "lin_values": bell_draw(key_of[7], (SEQUENCE_COUNT, SEQUENCE_LENGTH, W_LIN), 1.0, 6.0, ((0, 4), (1, 64), (2, 2))),
        "learn_logit": draw_learn_logit(jax.random.fold_in(key_of[13], 71), 0),
        "decay_log": draw_decay_log(jax.random.fold_in(key_of[13], 71), 0),
        "lin_gain": jnp.clip(1.0 + 0.18 * jax.random.normal(key_of[10], (W_LIN,), jnp.float32), 0.1, 1.9),
        "out_fox_weight": bell_draw(key_of[11], (W_FOX, D), (W_FOX + W_LIN) ** -0.5, 0.1875, ((0, 2), (1, 4))),
        "out_lin_weight": bell_draw(key_of[12], (W_LIN, D), (W_FOX + W_LIN) ** -0.5, 0.1875, ((0, 2), (1, 4))),
    }


HIGHEST = lax.Precision.HIGHEST
NORM_EPS = 1e-06

def round_half(tensor):
    return lax.optimization_barrier(tensor.astype(jnp.bfloat16)).astype(jnp.float32)

def forget_attention(query_rows, key_rows, value_rows, forget_rows, fox_gain):
    length = query_rows.shape[0]
    group_size = FOX_HEADS // KEY_HEADS
    block_rows = math.gcd(length, 512)
    block_count = length // block_rows
    score_scale = HEAD ** (-0.5)
    query_all = query_rows.astype(jnp.float32).reshape(block_count, block_rows, KEY_HEADS, group_size, HEAD)
    key_all = key_rows.astype(jnp.float32).reshape(block_count, block_rows, KEY_HEADS, HEAD)
    value_all = value_rows.astype(jnp.float32).reshape(block_count, block_rows, KEY_HEADS, HEAD)
    forget_all = jnp.transpose(forget_rows.reshape(block_count, block_rows, KEY_HEADS, group_size), (0, 2, 3, 1))
    offsets = jnp.arange(block_rows, dtype=jnp.int32)

    def query_block(block_index):
        query_here = query_all[block_index]
        forget_here = forget_all[block_index]

        def key_block(other, running):
            running_max, totals, weighted = running
            scores = jnp.einsum('tkgd,skd->kgts', query_here, key_all[other], precision=HIGHEST) * score_scale
            scores = scores + forget_here[:, :, :, None] - forget_all[other][:, :, None, :]
            allowed = (other * block_rows + offsets)[None, :] <= (block_index * block_rows + offsets)[:, None]
            scores = jnp.where(allowed, scores, -jnp.inf)
            new_max = jnp.maximum(running_max, lax.optimization_barrier(jnp.max(scores, axis=-1)))
            rescale = jnp.exp(running_max - new_max)
            weights = jnp.exp(scores - new_max[..., None])
            totals = totals * rescale + lax.optimization_barrier(jnp.sum(weights, axis=-1))
            update = jnp.einsum('kgts,skd->kgtd', round_half(weights), value_all[other], precision=HIGHEST)
            weighted = weighted * rescale[..., None] + update
            return (new_max, totals, weighted)
        start_state = (jnp.full((KEY_HEADS, group_size, block_rows), -jnp.inf, jnp.float32), jnp.zeros((KEY_HEADS, group_size, block_rows), jnp.float32), jnp.zeros((KEY_HEADS, group_size, block_rows, HEAD), jnp.float32))
        running_max, totals, weighted = lax.fori_loop(0, block_index + 1, key_block, start_state)
        heads_out = weighted / totals[..., None]
        return jnp.transpose(heads_out, (2, 0, 1, 3)).reshape(block_rows, FOX_HEADS, HEAD)
    attended = lax.map(query_block, jnp.arange(block_count, dtype=jnp.int32)).reshape(length, FOX_HEADS, HEAD)
    normed = attended * lax.rsqrt(lax.optimization_barrier(jnp.mean(attended * attended, axis=-1, keepdims=True)) + NORM_EPS)
    return (normed * fox_gain.reshape(FOX_HEADS, HEAD)).reshape(length, W_FOX).astype(jnp.bfloat16)

def delta_attention(recept_rows, key_rows, value_rows, learn_rows, decay_rows, lin_gain):
    length = recept_rows.shape[0]
    head_shape = (length, LIN_HEADS, HEAD)
    recept_float = recept_rows.astype(jnp.float32).reshape(head_shape)
    key_float = key_rows.astype(jnp.float32).reshape(head_shape)
    value_float = value_rows.astype(jnp.float32).reshape(head_shape)
    learn_rate = jax.nn.sigmoid(learn_rows.astype(jnp.float32)).reshape(head_shape)
    unit_keys = key_float * lax.rsqrt(lax.optimization_barrier(jnp.sum(key_float * key_float, axis=-1, keepdims=True)) + NORM_EPS)
    decays = jnp.exp(-jnp.exp(decay_rows)).reshape(head_shape)

    def advance(state, inputs):
        recept_t, key_t, value_t, unit_t, rate_t, decay_t = inputs
        projected = jnp.einsum('hvk,hk->hv', state, unit_t, precision=HIGHEST)
        state = state * decay_t[:, None, :] - projected[:, :, None] * (unit_t * rate_t)[:, None, :] + value_t[:, :, None] * key_t[:, None, :]
        return (state, jnp.einsum('hvk,hk->hv', state, recept_t, precision=HIGHEST))
    start_state = jnp.zeros((LIN_HEADS, HEAD, HEAD), jnp.float32)
    _, readout = lax.scan(advance, start_state, (recept_float, key_float, value_float, unit_keys, learn_rate, decays))
    centred = readout - lax.optimization_barrier(jnp.mean(readout, axis=-1, keepdims=True))
    normed = centred * lax.rsqrt(lax.optimization_barrier(jnp.mean(centred * centred, axis=-1, keepdims=True)) + HEAD * 1e-05)
    return (normed * lin_gain.reshape(LIN_HEADS, HEAD)).reshape(length, W_LIN).astype(jnp.bfloat16)

def reference(queries, keys, values, forget_cache, fox_gain, receptance, lin_keys, lin_values, learn_logit, decay_log, lin_gain, out_fox_weight, out_lin_weight):
    fox_part = W_FOX // N_TP
    lin_part = W_LIN // N_TP

    def one_sequence(inputs):
        query_rows, key_rows, value_rows, forget_rows, recept_rows, lkey_rows, lvalue_rows, learn_rows, decay_rows = inputs
        fox_out = forget_attention(query_rows, key_rows, value_rows, forget_rows, fox_gain)
        lin_out = delta_attention(recept_rows, lkey_rows, lvalue_rows, learn_rows, decay_rows, lin_gain)
        mixed = jnp.zeros((fox_out.shape[0], D), jnp.float32)
        for slot_index in range(N_TP):
            fox_cols = slice(slot_index * fox_part, (slot_index + 1) * fox_part)
            lin_cols = slice(slot_index * lin_part, (slot_index + 1) * lin_part)
            partial_value = jnp.dot(fox_out[:, fox_cols], out_fox_weight[fox_cols], preferred_element_type=jnp.float32)
            partial_value = partial_value + jnp.dot(lin_out[:, lin_cols], out_lin_weight[lin_cols], preferred_element_type=jnp.float32)
            mixed = mixed + round_half(partial_value)
        return mixed.astype(jnp.bfloat16)
    return lax.map(one_sequence, (queries, keys, values, forget_cache, receptance, lin_keys, lin_values, learn_logit, decay_log))
```

```python
import functools

import jax
import jax.numpy as jnp
from jax import lax
from jax.experimental import pallas as pl
from jax.experimental.pallas import tpu as pltpu
from jax.sharding import Mesh
from jax.sharding import PartitionSpec as P

HEAD = 64
SPAN = 64
TOK = 256
HEADS = 4
WIDE = HEADS * HEAD
PACK = 640
CHUNK = PACK // 2
SP = ("sp_0", "sp_1")
SP_TP = ("sp_0", "sp_1", "tp")
NORM_EPS = 1e-06
LOW = -1e30
MESH = pl.DeviceIdType.MESH
F32 = jnp.float32
BF16 = jnp.bfloat16


def dot(a, b):
    return lax.dot_general(a, b, (((1,), (0,)), ((), ())), preferred_element_type=F32)


def dot_t(a, b):
    return lax.dot_general(a, b, (((1,), (1,)), ((), ())), preferred_element_type=F32)


def t_dot(a, b):
    return lax.dot_general(a, b, (((0,), (0,)), ((), ())), preferred_element_type=F32)


def iota(shape, dim):
    return lax.broadcasted_iota(jnp.int32, shape, dim)


def three_parts(x):
    high = x.astype(BF16).astype(F32)
    middle = (x - high).astype(BF16).astype(F32)
    return high, middle, x - high - middle


class Ring:
    def __init__(self, axis, size, buf, send, recv):
        self.axis, self.size, self.buf, self.send, self.recv = axis, size, buf, send, recv
        self.me = lax.axis_index(axis)

    def last(self, way, part):
        return self.size // 2 if way == part else (self.size - 1) // 2

    def origin(self, way, step):
        if way == 0:
            return lax.rem(self.me - step + self.size, self.size)
        return lax.rem(self.me + step, self.size)

    def copy(self, way, part, step):
        slot = self.origin(way, step - 1)
        piece = self.buf.at[slot, pl.ds(part * CHUNK, CHUNK)]
        to = lax.rem(self.me + (1 if way == 0 else self.size - 1), self.size)
        return pltpu.make_async_remote_copy(
            src_ref=piece,
            dst_ref=piece,
            send_sem=self.send.at[way, part, step],
            recv_sem=self.recv.at[part, slot],
            device_id={self.axis: to},
            device_id_type=MESH,
        )

    def arrived(self, way, part, step):
        slot = self.origin(way, step)
        piece = self.buf.at[slot, pl.ds(part * CHUNK, CHUNK)]
        pltpu.make_async_remote_copy(
            src_ref=piece,
            dst_ref=piece,
            send_sem=self.send.at[way, part, step],
            recv_sem=self.recv.at[part, slot],
            device_id={self.axis: self.origin(way, 1)},
            device_id_type=MESH,
        ).wait_recv()

    def hop(self, step):
        for part in range(2):
            for way in range(2):
                if 1 < step <= self.last(way, part) + 1:
                    self.arrived(way, part, step - 1)
                if step <= self.last(way, part):
                    self.copy(way, part, step).start()

    def drain(self):
        for part in range(2):
            for way in range(2):
                for step in range(1, self.last(way, part) + 1):
                    self.copy(way, part, step).wait_send()


def to_peer(src, dst, send, recv, axis, to):
    return pltpu.make_async_remote_copy(
        src_ref=src,
        dst_ref=dst,
        send_sem=send,
        recv_sem=recv,
        device_id={axis: to},
        device_id_type=MESH,
    )


def kernel(
    sizes,
    q_ref,
    k_ref,
    v_ref,
    f_ref,
    fgain_ref,
    r_ref,
    lk_ref,
    lv_ref,
    ll_ref,
    dl_ref,
    lgain_ref,
    wf_ref,
    wl_ref,
    out_ref,
    ybuf,
    zbuf,
    wbuf,
    osend_a,
    osend_b,
    oa,
    ob,
    sty,
    stz,
    psend,
    precv,
    mixin,
    ein,
    rin,
    eout,
    wout,
    grown,
    g_s,
    h_s,
    p_s,
    o_s,
    inside_decay,
    inside_map,
    ysend,
    yrecv,
    zsend,
    zrecv,
    wsend,
    wrecv,
    asend,
    arecv,
    bsend,
    brecv,
    tysend,
    tyrecv,
    tzsend,
    tzrecv,
    psem,
):
    n0, n1, nf = sizes
    z, y = lax.axis_index("sp_0"), lax.axis_index("sp_1")
    x, core = lax.axis_index("fs"), lax.axis_index("tp")
    lane128 = iota((TOK, 128), 1)

    forget = f_ref[...]
    low_lane = lane128 < HEAD

    def key_block(pair):
        keys = k_ref[...].astype(F32)
        if pair == 1:
            keys = pltpu.roll(keys, HEAD, 1)
        block = jnp.where(low_lane, keys, 0.0)
        for member in range(2):
            column = 2 * pair + member
            wide = jnp.broadcast_to(-forget[:, column : column + 1], (TOK, 128))
            for place, piece in enumerate(three_parts(wide)):
                block = jnp.where(lane128 == HEAD + 3 * member + place, piece, block)
        return block.astype(BF16)

    values_t = jnp.transpose(v_ref[...].astype(F32)).astype(BF16)
    queries = (q_ref[...].astype(F32) * 0.125).astype(BF16)
    ybuf[y, 0:TOK] = queries[:, :128]
    zbuf[z, 0:TOK] = queries[:, 128:]
    for pair, buf, slot in ((0, zbuf, z), (1, ybuf, y)):
        buf[slot, TOK : 2 * TOK] = key_block(pair)
        rows = slice(pair * HEAD, (pair + 1) * HEAD)
        buf[slot, 2 * TOK : 2 * TOK + HEAD] = values_t[rows, :128]
        buf[slot, 2 * TOK + HEAD : PACK] = values_t[rows, 128:]

    barrier = pltpu.get_barrier_semaphore()
    peers = [("sp_0", n0, z), ("sp_1", n1, y), ("fs", nf, x), ("tp", 2, core)]
    for axis, size, me in peers:
        for d in range(1, size):
            pl.semaphore_signal(
                barrier, inc=1, device_id={axis: lax.rem(me + d, size)}, device_id_type=MESH
            )
    pl.semaphore_wait(barrier, sum(size - 1 for _, size, _ in peers))

    rings = (Ring("sp_1", n1, ybuf, ysend, yrecv), Ring("sp_0", n0, zbuf, zsend, zrecv))

    def hop(step):
        for ring in rings:
            ring.hop(step)

    hop(1)

    def weight_copies(d):
        to = lax.rem(x + d, nf)
        return [
            to_peer(
                ref,
                wbuf.at[x, pl.ds(part * WIDE, WIDE)],
                wsend.at[d, part],
                wrecv.at[part, x],
                "fs",
                to,
            )
            for part, ref in enumerate((wf_ref, wl_ref))
        ]

    for d in range(1, nf):
        for copy in weight_copies(d):
            copy.start()
    wbuf[x, 0:WIDE] = wf_ref[...]
    wbuf[x, WIDE : 2 * WIDE] = wl_ref[...]

    row, col = iota((TOK, TOK), 0), iota((TOK, TOK), 1)
    same_span = (row // SPAN) == (col // SPAN)
    same_head = same_span
    strict = jnp.logical_and(same_span, row > col)
    lower = jnp.logical_and(same_span, row >= col)
    head_ones = same_head.astype(F32).astype(BF16)

    def head_sum(t):
        high = t.astype(BF16)
        rest = (t - high.astype(F32)).astype(BF16)
        return dot(high, head_ones) + dot(rest, head_ones)

    lkeys = lk_ref[...].astype(F32)
    unit = lkeys * lax.rsqrt(head_sum(lkeys * lkeys) + NORM_EPS)
    fall = -jnp.exp(dl_ref[...])
    lower_ones = lower.astype(F32).astype(BF16)
    inclusive = sum(dot(lower_ones, piece.astype(BF16)) for piece in three_parts(fall))
    grow = jnp.exp(inclusive)
    shrink = jnp.exp(-inclusive)
    grown[...] = grow
    ein[...] = (-unit * jnp.exp(inclusive - fall)).astype(BF16)
    rin[...] = r_ref[...].astype(F32) * grow
    eout[...] = unit * jax.nn.sigmoid(ll_ref[...].astype(F32)) * shrink
    wout[...] = lkeys * shrink

    hops = n0 // 2 if n0 > n1 else n1 // 2
    for head in range(HEADS):
        in_head = (iota((TOK, WIDE), 1) // HEAD) == head

        def of_head(t):
            return jnp.where(in_head, t.astype(F32), 0.0).astype(BF16)

        e_in = ein[...]
        r_in = rin[...].astype(BF16)
        e_out = of_head(eout[...])
        w_out = of_head(wout[...])
        vals = of_head(lv_ref[...])
        mix_erase = jnp.where(strict, dot_t(e_in, e_out), 0.0)
        mix_write = jnp.where(strict, dot_t(e_in, w_out), 0.0).astype(BF16)
        read_erase = jnp.where(lower, dot_t(r_in, e_out), 0.0).astype(BF16)
        read_write = jnp.where(lower, dot_t(r_in, w_out), 0.0).astype(BF16)

        def level(size):
            odd = jnp.logical_and((row // size) % 2 == 1, (col // size) == (row // size) - 1)
            return jnp.where(odd, mix_erase, 0.0)

        inverse = jnp.where(row == col, 1.0, level(1))
        for size in (2, 4, 8, 16, 32):
            rounded = inverse.astype(BF16)
            step = dot(level(size).astype(BF16), rounded).astype(BF16)
            inverse = inverse + dot(rounded, step)
        inverse = inverse.astype(BF16)
        g_h = dot(inverse, of_head(e_in))
        h_h = dot(inverse, dot(mix_write, vals).astype(BF16))
        p_h = dot(read_erase, g_h.astype(BF16))
        o_h = dot(read_erase, h_h.astype(BF16)) + dot(read_write, vals)
        if head == 0:
            g_s[...], h_s[...], p_s[...], o_s[...] = g_h, h_h, rin[...] + p_h, o_h
        else:
            g_s[...] += g_h
            h_s[...] += h_h
            p_s[...] += p_h
            o_s[...] += o_h
        if head + 2 <= hops + 1:
            hop(head + 2)
    for step in range(HEADS + 2, hops + 2):
        hop(step)

    def compact(t):
        return t[0:64] + t[64:128] + t[128:192] + t[192:256]

    def expand(t):
        return jnp.where(same_head, jnp.concatenate([t.astype(F32)] * 4, axis=0), 0.0).astype(BF16)

    diagonal = iota((64, WIDE), 0) == iota((64, WIDE), 1) % HEAD

    def after(earlier, decay, change, added):
        before_decay, before = earlier
        left = before + jnp.concatenate(
            [jnp.where(diagonal, before_decay, 0.0), jnp.zeros((64, WIDE), F32)], axis=0
        )
        grown_by = jnp.concatenate([jnp.zeros((64, WIDE), F32), added], axis=0)
        return before_decay * decay, before * decay + dot(left.astype(BF16), change) + grown_by

    def put_map(ref, slot, decay, both):
        ref[slot, 0:128] = both.astype(BF16)
        place = iota((16, WIDE), 0)
        tail = jnp.zeros((16, WIDE), F32)
        for k, piece in enumerate(three_parts(decay)):
            tail = jnp.where(place == k, piece, tail)
        ref[slot, 128:144] = tail.astype(BF16)

    def get_map(ref, slot):
        tail = ref[slot, 128:144].astype(F32)
        return tail[0:1] + tail[1:2] + tail[2:3], ref[slot, 0:64], ref[slot, 64:128].astype(F32)

    for span in range(TOK // SPAN):
        at = slice(span * SPAN, (span + 1) * SPAN)
        final = grown[at.stop - 1 : at.stop, :]
        e_f = (eout[at, :] * final).astype(BF16)
        w_f = (wout[at, :] * final).astype(BF16)
        change = jnp.where(same_head, t_dot(g_s[at, :].astype(BF16), e_f), 0.0)
        added = t_dot(h_s[at, :].astype(BF16), e_f) + t_dot(lv_ref[at, :], w_f)
        added = compact(jnp.where(same_head, added, 0.0))
        if span == 0:
            chain = (final, jnp.concatenate([compact(change), added], axis=0))
        else:
            p_span = p_s[at, :].astype(BF16)
            o_s[at, :] += dot_t(p_span, expand(chain[1][64:128]))
            p_s[at, :] = p_s[at, :] * chain[0] + dot_t(p_span, expand(chain[1][0:64]))
            chain = after(chain, final, change.astype(BF16), added)
    put_map(sty, y, *chain)

    def row_copy(d):
        to = lax.rem(y + d, n1)
        return to_peer(sty.at[y], sty.at[y], tysend.at[d], tyrecv.at[y], "sp_1", to)

    for d in range(1, n1):
        row_copy(d).start()

    def query_pair(raw):
        wide = raw.astype(F32)
        ones = [
            jnp.where(
                jnp.logical_and(lane128 >= HEAD + 3 * m, lane128 < HEAD + 3 * m + 3), 1.0, 0.0
            )
            for m in range(2)
        ]
        first = jnp.where(low_lane, wide, ones[0])
        second = jnp.where(low_lane, pltpu.roll(wide, HEAD, 1), ones[1])
        return jnp.concatenate([first, second], axis=0).astype(BF16)

    def tile(q_pair, buf, slot, carry, masked):
        top, total, acc = carry
        scores = dot_t(buf[slot, TOK : 2 * TOK], q_pair)
        if masked:
            allowed = iota((TOK, 2 * TOK), 0) <= iota((TOK, 2 * TOK), 1) % TOK
            scores = jnp.where(allowed, scores, LOW)
        new_top = jnp.maximum(top, jnp.max(scores, axis=0, keepdims=True))
        scale = jnp.exp(top - new_top)
        weights = jnp.exp(scores - new_top)
        total = total * scale + jnp.sum(weights, axis=0, keepdims=True)
        vals = jnp.concatenate(
            [buf[slot, 2 * TOK : 2 * TOK + HEAD], buf[slot, 2 * TOK + HEAD : PACK]], axis=1
        )
        acc = acc * scale + dot(vals, weights.astype(BF16))
        return new_top, total, acc

    empty = (
        jnp.full((1, 2 * TOK), LOW, F32),
        jnp.zeros((1, 2 * TOK), F32),
        jnp.zeros((HEAD, 2 * TOK), F32),
    )

    def packed(carry):
        top, total, acc = carry
        some = total > 0.0
        acc = acc * jnp.where(some, 1.0 / jnp.where(some, total, 1.0), 0.0)
        level = jnp.where(some, top + jnp.log(jnp.where(some, total, 1.0)), LOW)
        place = iota((16, TOK), 0)
        tail = jnp.zeros((16, TOK), F32)
        for member in range(2):
            part = level[:, member * TOK : (member + 1) * TOK]
            for k, piece in enumerate(three_parts(part)):
                tail = jnp.where(place == 3 * member + k, piece, tail)
        return acc.astype(BF16), tail.astype(BF16)

    def put(ref, slot, carry):
        acc, tail = packed(carry)
        ref[slot, 0:HEAD] = acc[:, :TOK]
        ref[slot, HEAD : 2 * HEAD] = acc[:, TOK:]
        ref[slot, 2 * HEAD : 2 * HEAD + 16] = tail

    def attend(size, me, axis, q_buf, kv_buf, kv_me, count_of, keep, stage, send, recv):
        def one(d, masked):
            block = lax.rem(me + d, size)
            q_pair = query_pair(q_buf[block, 0:TOK])
            start = tile(q_pair, kv_buf, kv_me, empty, True) if masked else empty
            return lax.fori_loop(
                0,
                count_of(block),
                lambda slot, carry: tile(q_pair, kv_buf, slot, carry, False),
                start,
            )

        def others(d, _):
            to = lax.rem(me + d, size)
            put(stage, d, one(d, False))
            to_peer(stage.at[d], keep.at[me], send.at[d], recv.at[me], axis, to).start()
            return 0

        lax.fori_loop(1, size, others, 0)
        put(keep, me, one(0, True))

    def count_a(block):
        return z + jnp.where(y < block, 1, 0)

    def count_b(block):
        return jnp.where(block > z, n1, jnp.where(block == z, y, 0))

    attend(n1, y, "sp_1", ybuf, zbuf, z, count_a, oa, osend_a, asend, arecv)

    def row_arrived(d, _):
        slot = lax.rem(y + d, n1)
        to_peer(sty.at[slot], sty.at[slot], tysend.at[d], tyrecv.at[slot], "sp_1", slot).wait_recv()
        return 0

    lax.fori_loop(1, n1, row_arrived, 0)
    @pl.when(y == 0)
    def _():
        inside_decay[...] = jnp.ones((8, WIDE), F32)
        inside_map[...] = jnp.zeros((128, WIDE), F32)

    def follow(k, so_far):
        @pl.when(k == y)
        def _():
            inside_decay[...] = jnp.broadcast_to(so_far[0], (8, WIDE))
            inside_map[...] = so_far[1]

        decay, change, added = get_map(sty, k)
        return after(so_far, decay, expand(change), added)

    decay, change, added = get_map(sty, 0)
    first = (decay, jnp.concatenate([change.astype(F32), added], axis=0))
    whole = lax.fori_loop(1, n1, follow, first)
    put_map(stz, z, *whole)

    def column_copy(d):
        return to_peer(stz.at[z], stz.at[z], tzsend.at[d], tzrecv.at[z], "sp_0", lax.rem(z + d, n0))

    def column_send(d, _):
        column_copy(d).start()
        return 0

    lax.fori_loop(1, n0 - z, column_send, 0)

    attend(n0, z, "sp_0", zbuf, ybuf, y, count_b, ob, osend_b, bsend, brecv)

    def column_arrived(slot, _):
        to_peer(stz.at[slot], stz.at[slot], tzsend.at[0], tzrecv.at[slot], "sp_0", slot).wait_recv()
        return 0

    lax.fori_loop(0, z, column_arrived, 0)

    def enter(k, state):
        decay, change, added = get_map(stz, k)
        return state * decay + dot(state.astype(BF16), expand(change)) + added

    entry = lax.fori_loop(0, z, enter, jnp.zeros((64, WIDE), F32))
    entry = (
        entry * inside_decay[0:1, :]
        + dot(entry.astype(BF16), expand(inside_map[0:64, :]))
        + inside_map[64:128, :]
    )
    read = o_s[...] + dot_t(p_s[...].astype(BF16), expand(entry))
    centred = read - head_sum(read) * (1.0 / HEAD)
    normed = centred * lax.rsqrt(head_sum(centred * centred) * (1.0 / HEAD) + HEAD * 1e-05)
    mixin[:, WIDE:] = (normed * lgain_ref[...]).astype(BF16)

    def joined(size, me, keep, send, recv, axis):
        def wait(d, _):
            slot = lax.rem(me + d, size)
            to_peer(keep.at[slot], keep.at[slot], send.at[d], recv.at[slot], axis, slot).wait_recv()
            return 0

        lax.fori_loop(1, size, wait, 0)
        levels = []
        for slot in range(size):
            tail = keep[slot, 2 * HEAD : 2 * HEAD + 16].astype(F32)
            levels.append(
                [tail[3 * m : 3 * m + 1] + tail[3 * m + 1 : 3 * m + 2] + tail[3 * m + 2 : 3 * m + 3] for m in range(2)]
            )
        heads = []
        for member in range(2):
            top = functools.reduce(jnp.maximum, [l[member] for l in levels])
            total, acc = 0.0, 0.0
            for slot in range(size):
                part = jnp.exp(levels[slot][member] - top)
                total = total + part
                acc = acc + part * keep[slot, member * HEAD : (member + 1) * HEAD].astype(F32)
            acc = acc * (1.0 / total)
            square = jnp.sum(acc * acc, axis=0, keepdims=True) * (1.0 / HEAD)
            heads.append(acc * lax.rsqrt(square + NORM_EPS))
        return jnp.concatenate(heads, axis=0)

    mixed = jnp.concatenate(
        [joined(n1, y, oa, asend, arecv, "sp_1"), joined(n0, z, ob, bsend, brecv, "sp_0")], axis=0
    )
    mixin[:, :WIDE] = (jnp.transpose(mixed) * fgain_ref[...]).astype(BF16)

    for d in range(1, nf):
        slot = lax.rem(x + d, nf)
        for part in range(2):
            piece = wbuf.at[slot, pl.ds(part * WIDE, WIDE)]
            to_peer(piece, piece, wsend.at[d, part], wrecv.at[part, slot], "fs", slot).wait_recv()
    half = TOK // 2
    columns = wf_ref.shape[1]
    partner = 1 - core
    theirs = mixin[pl.ds(pl.multiple_of(partner * half, half), half), :]
    for slot in range(nf):
        at = slice(slot * columns, (slot + 1) * columns)
        psend[:, at] = dot(theirs, wbuf[slot]).astype(BF16)
    swap = to_peer(psend, precv, psem.at[0], psem.at[1], "tp", partner)
    swap.start()
    mine = mixin[pl.ds(pl.multiple_of(core * half, half), half), :]
    for slot in range(nf):
        at = slice(slot * columns, (slot + 1) * columns)
        out_ref[:, at] = dot(mine, wbuf[slot]).astype(BF16)
    swap.wait()
    out_ref[...] = (out_ref[...].astype(F32) + precv[...].astype(F32)).astype(BF16)

    for ring in rings:
        ring.drain()
    for d in range(1, nf):
        for copy in weight_copies(d):
            copy.wait_send()
    for d in range(1, n1):
        row_copy(d).wait_send()

    def column_left(d, _):
        column_copy(d).wait_send()
        return 0

    lax.fori_loop(1, n0 - z, column_left, 0)

    def left(size, me, keep, stage, send, recv, axis):
        def one(d, _):
            to = lax.rem(me + d, size)
            to_peer(stage.at[d], keep.at[me], send.at[d], recv.at[me], axis, to).wait_send()
            return 0

        lax.fori_loop(1, size, one, 0)

    left(n1, y, oa, osend_a, asend, arecv, "sp_1")
    left(n0, z, ob, osend_b, bsend, brecv, "sp_0")


def solution(mesh):
    nf, n_tp = mesh.shape["fs"], mesh.shape["tp"]
    n0 = 8 if mesh.shape["sp"] == 64 else mesh.shape["sp"] // 2
    n1 = mesh.shape["sp"] // n0
    finer = Mesh(mesh.devices.reshape(n0, n1, nf, n_tp), ("sp_0", "sp_1", "fs", "tp"))

    def shards(q, k, v, f, fgain, r, lk, lv, ll, dl, lgain, wf, wl):
        width = wf.shape[1] * nf
        vm = pl.BlockSpec(memory_space=pltpu.VMEM)
        dma = pltpu.SemaphoreType.DMA
        wide32 = pltpu.VMEM((TOK, WIDE), F32)
        part = (2 * HEAD + 16, TOK)
        out = pl.pallas_call(
            functools.partial(kernel, (n0, n1, nf)),
            out_shape=jax.ShapeDtypeStruct((TOK // 2, width), BF16),
            in_specs=[vm] * 13,
            out_specs=vm,
            scratch_shapes=[
                pltpu.VMEM((n1, PACK, 128), BF16),
                pltpu.VMEM((n0, PACK, 128), BF16),
                pltpu.VMEM((nf, 2 * WIDE, wf.shape[1]), BF16),
                pltpu.VMEM((n1, *part), BF16),
                pltpu.VMEM((n0, *part), BF16),
                pltpu.VMEM((n1, *part), BF16),
                pltpu.VMEM((n0, *part), BF16),
                pltpu.VMEM((n1, 144, WIDE), BF16),
                pltpu.VMEM((n0, 144, WIDE), BF16),
                pltpu.VMEM((TOK // 2, width), BF16),
                pltpu.VMEM((TOK // 2, width), BF16),
                pltpu.VMEM((TOK, 2 * WIDE), BF16),
                pltpu.VMEM((TOK, WIDE), BF16),
                wide32,
                wide32,
                wide32,
                wide32,
                wide32,
                wide32,
                wide32,
                wide32,
                pltpu.VMEM((8, WIDE), F32),
                pltpu.VMEM((128, WIDE), F32),
                dma((2, 2, n1 // 2 + 1)),
                dma((2, n1)),
                dma((2, 2, n0 // 2 + 1)),
                dma((2, n0)),
                dma((nf, 2)),
                dma((2, nf)),
                dma((n1,)),
                dma((n1,)),
                dma((n0,)),
                dma((n0,)),
                dma((n1,)),
                dma((n1,)),
                dma((n0,)),
                dma((n0,)),
                dma((2,)),
            ],
            compiler_params=pltpu.CompilerParams(
                collective_id=0, has_side_effects=True, vmem_limit_bytes=60 * 1024 * 1024
            ),
        )(
            q[0], k[0], v[0], f[0], fgain[None], r[0], lk[0], lv[0], ll[0], dl[0], lgain[None], wf, wl
        )
        return out[None]

    heads = P("fs", SP, "tp")
    gains, weights = P("tp"), P("tp", "fs")
    placed = (heads,) * 4 + (gains,) + (heads,) * 5 + (gains, weights, weights)
    return jax.shard_map(
        shards, mesh=finer, in_specs=placed, out_specs=P("fs", SP_TP, None), check_vma=False
    )
```

```python
import functools

import jax
import jax.numpy as jnp
from jax import lax
from jax.experimental import pallas as pl
from jax.experimental.pallas import tpu as pltpu
from jax.sharding import Mesh
from jax.sharding import PartitionSpec as P

HEAD = 64
SPAN = 64
TOK = 256
HEADS = 4
WIDE = HEADS * HEAD
PACK = 640
CHUNK = PACK // 2
SP = ("sp_0", "sp_1")
SP_TP = ("sp_0", "sp_1", "tp")
NORM_EPS = 1e-06
LOW = -1e30
MESH = pl.DeviceIdType.MESH
F32 = jnp.float32
BF16 = jnp.bfloat16


def dot(a, b):
    return lax.dot_general(a, b, (((1,), (0,)), ((), ())), preferred_element_type=F32)


def dot_t(a, b):
    return lax.dot_general(a, b, (((1,), (1,)), ((), ())), preferred_element_type=F32)


def t_dot(a, b):
    return lax.dot_general(a, b, (((0,), (0,)), ((), ())), preferred_element_type=F32)


def iota(shape, dim):
    return lax.broadcasted_iota(jnp.int32, shape, dim)


def three_parts(x):
    high = x.astype(BF16).astype(F32)
    middle = (x - high).astype(BF16).astype(F32)
    return high, middle, x - high - middle


class Ring:
    def __init__(self, axis, size, buf, send, recv):
        self.axis, self.size, self.buf, self.send, self.recv = axis, size, buf, send, recv
        self.me = lax.axis_index(axis)

    def last(self, way, part):
        return self.size // 2 if way == part else (self.size - 1) // 2

    def origin(self, way, step):
        if way == 0:
            return lax.rem(self.me - step + self.size, self.size)
        return lax.rem(self.me + step, self.size)

    def copy(self, way, part, step):
        slot = self.origin(way, step - 1)
        piece = self.buf.at[slot, pl.ds(part * CHUNK, CHUNK)]
        to = lax.rem(self.me + (1 if way == 0 else self.size - 1), self.size)
        return pltpu.make_async_remote_copy(
            src_ref=piece,
            dst_ref=piece,
            send_sem=self.send.at[way, part, step],
            recv_sem=self.recv.at[part, slot],
            device_id={self.axis: to},
            device_id_type=MESH,
        )

    def arrived(self, way, part, step):
        slot = self.origin(way, step)
        piece = self.buf.at[slot, pl.ds(part * CHUNK, CHUNK)]
        pltpu.make_async_remote_copy(
            src_ref=piece,
            dst_ref=piece,
            send_sem=self.send.at[way, part, step],
            recv_sem=self.recv.at[part, slot],
            device_id={self.axis: self.origin(way, 1)},
            device_id_type=MESH,
        ).wait_recv()

    def hop(self, step, part):
        for way in range(2):
            if 1 < step <= self.last(way, part) + 1:
                self.arrived(way, part, step - 1)
            if step <= self.last(way, part):
                self.copy(way, part, step).start()

    def drain(self):
        for part in range(2):
            for way in range(2):
                for step in range(1, self.last(way, part) + 1):
                    self.copy(way, part, step).wait_send()


def to_peer(src, dst, send, recv, axis, to):
    return pltpu.make_async_remote_copy(
        src_ref=src,
        dst_ref=dst,
        send_sem=send,
        recv_sem=recv,
        device_id={axis: to},
        device_id_type=MESH,
    )


def kernel(
    sizes,
    q_ref,
    k_ref,
    v_ref,
    f_ref,
    fgain_ref,
    r_ref,
    lk_ref,
    lv_ref,
    ll_ref,
    dl_ref,
    lgain_ref,
    wf_ref,
    wl_ref,
    out_ref,
    both,
    wbuf,
    pairs,
    accs,
    tops,
    osend,
    okeep,
    hsend,
    hkeep,
    zkeep,
    esend,
    ekeep,
    psend,
    precv,
    mixin,
    ein,
    rin,
    eout,
    wout,
    grown,
    g_s,
    h_s,
    p_s,
    o_s,
    inside,
    ysend,
    yrecv,
    zsend,
    zrecv,
    wsend,
    wrecv,
    osem_send,
    osem_recv,
    hsem_send,
    hsem_recv,
    zsem_send,
    zsem_recv,
    esem_send,
    esem_recv,
    psem,
):
    n0, n1, nf = sizes
    z, y = lax.axis_index("sp_0"), lax.axis_index("sp_1")
    x, core = lax.axis_index("fs"), lax.axis_index("tp")
    lane128 = iota((TOK, 128), 1)

    low_lane = lane128 < HEAD
    ybuf, zbuf = both.at[0], both.at[1]

    def key_block(pair):
        keys = k_ref[...].astype(F32)
        if pair == 1:
            keys = pltpu.roll(keys, HEAD, 1)
        place = iota((128, TOK), 0)
        gates = jnp.zeros((128, TOK), F32)
        for member in range(2):
            line = -f_ref[2 * pair + member : 2 * pair + member + 1, :]
            for k, piece in enumerate(three_parts(line)):
                gates = jnp.where(place == HEAD + 3 * member + k, piece, gates)
        return jnp.where(low_lane, keys, jnp.transpose(gates)).astype(BF16)

    values_t = jnp.transpose(v_ref[...].astype(F32)).astype(BF16)
    queries = (q_ref[...].astype(F32) * 0.125).astype(BF16)
    ybuf[y, 0:TOK] = queries[:, :128]
    zbuf[z, 0:TOK] = queries[:, 128:]
    for pair, buf, slot in ((0, zbuf, z), (1, ybuf, y)):
        buf[slot, TOK : 2 * TOK] = key_block(pair)
        rows = slice(pair * HEAD, (pair + 1) * HEAD)
        buf[slot, 2 * TOK : 2 * TOK + HEAD] = values_t[rows, :128]
        buf[slot, 2 * TOK + HEAD : PACK] = values_t[rows, 128:]

    barrier = pltpu.get_barrier_semaphore()
    peers = [("sp_0", n0, z), ("sp_1", n1, y), ("fs", nf, x), ("tp", 2, core)]
    for axis, size, me in peers:
        for d in range(1, size):
            pl.semaphore_signal(
                barrier, inc=1, device_id={axis: lax.rem(me + d, size)}, device_id_type=MESH
            )
    pl.semaphore_wait(barrier, sum(size - 1 for _, size, _ in peers))

    rings = (Ring("sp_1", n1, ybuf, ysend, yrecv), Ring("sp_0", n0, zbuf, zsend, zrecv))

    def hop(step):
        for part in range(2):
            for ring in rings:
                ring.hop(step, part)

    hop(1)

    def weight_copies(d):
        to = lax.rem(x + d, nf)
        return [
            to_peer(
                ref,
                wbuf.at[x, pl.ds(part * WIDE, WIDE)],
                wsend.at[d, part],
                wrecv.at[part, x],
                "fs",
                to,
            )
            for part, ref in enumerate((wf_ref, wl_ref))
        ]

    row, col = iota((TOK, TOK), 0), iota((TOK, TOK), 1)
    same_span = (row // SPAN) == (col // SPAN)
    same_head = same_span
    strict = jnp.logical_and(same_span, row > col)
    lower = jnp.logical_and(same_span, row >= col)
    head_ones = same_head.astype(F32).astype(BF16)

    def head_sum(t):
        high = t.astype(BF16)
        rest = (t - high.astype(F32)).astype(BF16)
        return dot(high, head_ones) + dot(rest, head_ones)

    lkeys = lk_ref[...].astype(F32)
    unit = lkeys * lax.rsqrt(head_sum(lkeys * lkeys) + NORM_EPS)
    fall = -jnp.exp(dl_ref[...])
    lower_ones = lower.astype(F32).astype(BF16)
    inclusive = sum(dot(lower_ones, piece.astype(BF16)) for piece in three_parts(fall))
    grow = jnp.exp(inclusive)
    shrink = jnp.exp(-inclusive)
    grown[...] = grow
    ein[...] = (-unit * jnp.exp(inclusive - fall)).astype(BF16)
    rin[...] = r_ref[...].astype(F32) * grow
    eout[...] = unit * jax.nn.sigmoid(ll_ref[...].astype(F32)) * shrink
    wout[...] = lkeys * shrink

    for head in range(HEADS):
        in_head = (iota((TOK, WIDE), 1) // HEAD) == head

        def of_head(t):
            return jnp.where(in_head, t.astype(F32), 0.0).astype(BF16)

        e_in = ein[...]
        r_in = rin[...].astype(BF16)
        e_out = of_head(eout[...])
        w_out = of_head(wout[...])
        vals = of_head(lv_ref[...])
        mix_erase = jnp.where(strict, dot_t(e_in, e_out), 0.0)
        mix_write = jnp.where(strict, dot_t(e_in, w_out), 0.0).astype(BF16)
        read_erase = jnp.where(lower, dot_t(r_in, e_out), 0.0).astype(BF16)
        read_write = jnp.where(lower, dot_t(r_in, w_out), 0.0).astype(BF16)

        def level(size):
            odd = jnp.logical_and((row // size) % 2 == 1, (col // size) == (row // size) - 1)
            return jnp.where(odd, mix_erase, 0.0)

        inverse = jnp.where(row == col, 1.0, level(1))
        for size in (2, 4, 8, 16, 32):
            rounded = inverse.astype(BF16)
            step = dot(level(size).astype(BF16), rounded).astype(BF16)
            inverse = inverse + dot(rounded, step)
        inverse = inverse.astype(BF16)
        g_h = dot(inverse, of_head(e_in))
        h_h = dot(inverse, dot(mix_write, vals).astype(BF16))
        p_h = dot(read_erase, g_h.astype(BF16))
        o_h = dot(read_erase, h_h.astype(BF16)) + dot(read_write, vals)
        if head == 0:
            g_s[...], h_s[...], p_s[...], o_s[...] = g_h, h_h, rin[...] + p_h, o_h
        else:
            g_s[...] += g_h
            h_s[...] += h_h
            p_s[...] += p_h
            o_s[...] += o_h
        if head == 1:
            hop(2)

    def compact(t):
        return t[0:64] + t[64:128] + t[128:192] + t[192:256]

    def expand(t):
        copies = t.shape[1] // HEAD
        wide = jnp.concatenate([t.astype(F32)] * copies, axis=0)
        return jnp.where(same_head[: wide.shape[0], : wide.shape[1]], wide, 0.0).astype(BF16)

    def after(earlier, decay, change, added):
        before_decay, before = earlier
        width, rows = before.shape[1], added.shape[0]
        diagonal = iota((64, width), 0) == iota((64, width), 1) % HEAD
        left = before + jnp.concatenate(
            [jnp.where(diagonal, before_decay, 0.0), jnp.zeros((rows, width), F32)], axis=0
        )
        grown_by = jnp.concatenate([jnp.zeros((64, width), F32), added], axis=0)
        return before_decay * decay, before * decay + dot(left.astype(BF16), change) + grown_by

    def decay_rows(decay):
        place = iota((16, decay.shape[1]), 0)
        tail = jnp.zeros((16, decay.shape[1]), F32)
        for k, piece in enumerate(three_parts(decay)):
            tail = jnp.where(place == k, piece, tail)
        return tail.astype(BF16)

    def get_map(t):
        tail = t[80:96].astype(F32)
        return tail[0:1] + tail[1:2] + tail[2:3], t[0:64], t[64:80].astype(F32)

    for span in range(TOK // SPAN):
        at = slice(span * SPAN, (span + 1) * SPAN)
        final = grown[at.stop - 1 : at.stop, :]
        e_f = (eout[at, :] * final).astype(BF16)
        w_f = (wout[at, :] * final).astype(BF16)
        change = jnp.where(same_head, t_dot(g_s[at, :].astype(BF16), e_f), 0.0)
        added = t_dot(h_s[at, :].astype(BF16), e_f) + t_dot(lv_ref[at, :], w_f)
        added = compact(jnp.where(same_head, added, 0.0))
        if span == 0:
            chain = (final, jnp.concatenate([compact(change), added], axis=0))
        else:
            p_span = p_s[at, :].astype(BF16)
            o_s[at, :] += dot_t(p_span, expand(chain[1][64:128]))
            p_s[at, :] = p_s[at, :] * chain[0] + dot_t(p_span, expand(chain[1][0:64]))
            chain = after(chain, final, change.astype(BF16), added)
    for u in range(n1):
        lanes, rows = slice((u // 4) * 128, (u // 4 + 1) * 128), 64 + 16 * (u % 4)
        hsend[u, 0:64] = chain[1][0:64, lanes].astype(BF16)
        hsend[u, 64:80] = chain[1][rows : rows + 16, lanes].astype(BF16)
        hsend[u, 80:96] = decay_rows(chain[0][:, lanes])
    hkeep[y] = hsend[y]

    def handler_copy(d):
        to = lax.rem(y + d, n1)
        return to_peer(
            hsend.at[to], hkeep.at[y], hsem_send.at[d], hsem_recv.at[y], "sp_1", to
        )

    def entry_copy(d):
        to = lax.rem(y + d, n1)
        return to_peer(
            esend.at[to], ekeep.at[y], esem_send.at[d], esem_recv.at[y], "sp_1", to
        )

    def column_copy(d):
        to = lax.rem(z + d, n0)
        return to_peer(zkeep.at[z], zkeep.at[z], zsem_send.at[d], zsem_recv.at[z], "sp_0", to)

    def from_row(keep, send, recv):
        def one(d, _):
            slot = lax.rem(y + d, n1)
            to_peer(keep.at[slot], keep.at[slot], send.at[d], recv.at[slot], "sp_1", slot).wait_recv()
            return 0

        lax.fori_loop(1, n1, one, 0)

    def states_row():
        from_row(hkeep, hsem_send, hsem_recv)
        decay, change, added = get_map(hkeep[0])
        first = (decay, jnp.concatenate([change.astype(F32), added], axis=0))

        def follow(k, so_far):
            inside[k, 0:80] = so_far[1]
            inside[k, 80:88] = jnp.broadcast_to(so_far[0], (8, 128))
            decay, change, added = get_map(hkeep[k])
            return after(so_far, decay, expand(change), added)

        decay, whole = lax.fori_loop(1, n1, follow, first)
        zkeep[z, 0:80] = whole.astype(BF16)
        zkeep[z, 80:96] = decay_rows(decay)

        def send(d, _):
            column_copy(d).start()
            return 0

        lax.fori_loop(1, n0 - z, send, 0)

    def states_column():
        def arrived(slot, _):
            to_peer(
                zkeep.at[slot], zkeep.at[slot], zsem_send.at[0], zsem_recv.at[slot], "sp_0", slot
            ).wait_recv()
            return 0

        lax.fori_loop(0, z, arrived, 0)

        def enter(k, state):
            decay, change, added = get_map(zkeep[k])
            return state * decay + dot(state.astype(BF16), expand(change)) + added

        entry = lax.fori_loop(0, z, enter, jnp.zeros((16, 128), F32))
        esend[0] = entry.astype(BF16)
        for k in range(1, n1):
            here = inside[k]
            moved = entry * here[80:81] + dot(entry.astype(BF16), expand(here[0:64]))
            esend[k] = (moved + here[64:80]).astype(BF16)
        ekeep[y] = esend[y]
        for d in range(1, n1):
            entry_copy(d).start()

    for d in range(1, n1):
        handler_copy(d).start()
    hop(3)
    for d in range(1, nf):
        for copy in weight_copies(d):
            copy.start()
    wbuf[x, 0:WIDE] = wf_ref[...]
    wbuf[x, WIDE : 2 * WIDE] = wl_ref[...]

    def query_pair(raw):
        wide = raw.astype(F32)
        ones = [
            jnp.where(
                jnp.logical_and(lane128 >= HEAD + 3 * m, lane128 < HEAD + 3 * m + 3), 1.0, 0.0
            )
            for m in range(2)
        ]
        first = jnp.where(low_lane, wide, ones[0])
        second = jnp.where(low_lane, pltpu.roll(wide, HEAD, 1), ones[1])
        return jnp.concatenate([first, second], axis=0).astype(BF16)

    def tile(q_pair, buf, slot, carry, masked=False):
        top, total, acc = carry
        scores = dot_t(buf[slot, TOK : 2 * TOK], q_pair)
        if masked:
            allowed = iota((TOK, 2 * TOK), 0) <= iota((TOK, 2 * TOK), 1) % TOK
            scores = jnp.where(allowed, scores, LOW)
        new_top = jnp.maximum(top, jnp.max(scores, axis=0, keepdims=True))
        scale = jnp.exp(top - new_top)
        weights = jnp.exp(scores - new_top)
        total = total * scale + jnp.sum(weights, axis=0, keepdims=True)
        vals = jnp.concatenate(
            [buf[slot, 2 * TOK : 2 * TOK + HEAD], buf[slot, 2 * TOK + HEAD : PACK]], axis=1
        )
        acc = acc * scale + dot(vals, weights.astype(BF16))
        return new_top, total, acc

    def load(group, block):
        return tops[group, block, 0:1], tops[group, block, 1:2], accs[group, block]

    def save(group, block, carry):
        tops[group, block, 0:1], tops[group, block, 1:2], accs[group, block] = carry

    def put(ref, group, slot, carry):
        top, total, acc = carry
        place = iota((16, TOK), 0)
        tail = jnp.zeros((16, TOK), F32)
        for which, line in enumerate((top, total)):
            for k, piece in enumerate(three_parts(line)):
                for member in range(2):
                    part = piece[:, member * TOK : (member + 1) * TOK]
                    tail = jnp.where(place == 6 * which + 3 * member + k, part, tail)
        acc = acc.astype(BF16)
        ref[group, slot, 0:HEAD] = acc[:, :TOK]
        ref[group, slot, HEAD : 2 * HEAD] = acc[:, TOK:]
        ref[group, slot, 2 * HEAD : 2 * HEAD + 16] = tail.astype(BF16)

    tops[:, :, 0:1] = jnp.full((2, tops.shape[1], 1, 2 * TOK), LOW, F32)
    tops[:, :, 1:2] = jnp.zeros((2, tops.shape[1], 1, 2 * TOK), F32)
    accs[...] = jnp.zeros(accs.shape, F32)
    reach0, reach1 = min(2, (n0 - 1) // 2), min(2, (n1 - 1) // 2)
    row_of, column_of = ("sp_1", n1, y, reach1), ("sp_0", n0, z, reach0)

    def make_pairs(group, first, count):
        axis, size, me, reach = (row_of, column_of)[group]

        def one(d, _):
            block = lax.rem(me + (first % size) + d, size)
            pairs[group, block] = query_pair(both[group, block, 0:TOK])
            return 0

        lax.fori_loop(0, count, one, 0)

    def near(skip0, skip1, far0, far1):
        across = 2 * far1 + 1

        def one(t, _):
            down, right = t // across, t % across
            inner = jnp.logical_and(
                jnp.logical_and(down >= far0 - skip0, down <= far0 + skip0),
                jnp.logical_and(right >= far1 - skip1, right <= far1 + skip1),
            )

            @pl.when(jnp.logical_not(inner))
            def _():
                i, j = lax.rem(z + down + (n0 - far0), n0), lax.rem(y + right + (n1 - far1), n1)
                first = jnp.logical_or(i < z, jnp.logical_and(i == z, y < j))
                group = jnp.where(first, 0, 1)
                block = jnp.where(first, j, i)
                slot = jnp.where(first, i, j)
                carry = load(group, block)
                save(group, block, tile(pairs[group, block], both.at[1 - group], slot, carry))

            return 0

        lax.fori_loop(0, (2 * far0 + 1) * across, one, 0)

    make_pairs(0, -reach1, 2 * reach1 + 1)
    make_pairs(1, -reach0, 2 * reach0 + 1)
    for group, me, slot in ((0, y, z), (1, z, y)):
        carry = load(group, me)
        save(group, me, tile(pairs[group, me], both.at[1 - group], slot, carry, True))
    near(0, 0, min(1, reach0), min(1, reach1))
    hop(4)
    near(min(1, reach0), min(1, reach1), reach0, reach1)
    states_row()
    hop(5)
    make_pairs(0, reach1 + 1, n1 - 2 * reach1 - 1)
    make_pairs(1, reach0 + 1, n0 - 2 * reach0 - 1)

    def rest(group, d):
        axis, size, me, reach = (row_of, column_of)[group]
        block = lax.rem(me + d, size)
        is_near = jnp.logical_or(d <= reach, d >= size - reach)
        if group == 0:
            start = jnp.maximum(jnp.where(is_near, reach0 + 1, 1), n0 - z)
            end = jnp.where(is_near, n0 - reach0, n0 + jnp.where(y < block, 1, 0))
            mine, count = z, n0
        else:
            start = jnp.where(is_near, reach1 + 1, 0)
            end = jnp.where(is_near, n1 - reach1, n1)
            start = jnp.where(d == 0, jnp.maximum(start, n1 - y), start)
            end = jnp.where(jnp.logical_and(d > 0, block < z), start, end)
            mine, count = y, n1
        q_pair = pairs[group, block]

        def one(t, carry):
            return tile(q_pair, both.at[1 - group], lax.rem(mine + t, count), carry)

        return lax.fori_loop(start, end, one, load(group, block))

    def output_copy(group, d):
        axis, size, me, reach = (row_of, column_of)[group]
        return to_peer(
            osend.at[group, d],
            okeep.at[group, me],
            osem_send.at[group, d],
            osem_recv.at[group, me],
            axis,
            lax.rem(me + d, size),
        )

    def finish(low, high):
        def one(d, _):
            for group, size in ((0, n1), (1, n0)):

                @pl.when(d < size)
                def _():
                    put(osend, group, d, rest(group, d))
                    output_copy(group, d).start()

            return 0

        lax.fori_loop(low, high, one, 0)

    longest = max(n0, n1)
    finish(1, min(4, longest))
    states_column()
    finish(min(4, longest), longest)
    put(okeep, 0, y, rest(0, 0))
    put(okeep, 1, z, rest(1, 0))

    from_row(ekeep, esem_send, esem_recv)
    entry = jnp.concatenate(
        [
            jnp.concatenate([ekeep[4 * tile_of + k] for k in range(4)], axis=0)
            for tile_of in range(2)
        ],
        axis=1,
    )
    read = o_s[...] + dot_t(p_s[...].astype(BF16), expand(entry))
    centred = read - head_sum(read) * (1.0 / HEAD)
    normed = centred * lax.rsqrt(head_sum(centred * centred) * (1.0 / HEAD) + HEAD * 1e-05)
    mixin[:, WIDE:] = (normed * lgain_ref[...]).astype(BF16)

    def joined(group):
        axis, size, me, reach = (row_of, column_of)[group]

        def wait(d, _):
            slot = lax.rem(me + d, size)
            piece = okeep.at[group, slot]
            to_peer(
                piece, piece, osem_send.at[group, d], osem_recv.at[group, slot], axis, slot
            ).wait_recv()
            return 0

        lax.fori_loop(1, size, wait, 0)
        lines = []
        for slot in range(size):
            tail = okeep[group, slot, 2 * HEAD : 2 * HEAD + 16].astype(F32)
            lines.append([tail[3 * k : 3 * k + 1] + tail[3 * k + 1 : 3 * k + 2] + tail[3 * k + 2 : 3 * k + 3] for k in range(4)])
        heads = []
        for member in range(2):
            top = functools.reduce(jnp.maximum, [line[member] for line in lines])
            total, acc = 0.0, 0.0
            for slot in range(size):
                scale = jnp.exp(lines[slot][member] - top)
                total = total + scale * lines[slot][2 + member]
                part = okeep[group, slot, member * HEAD : (member + 1) * HEAD]
                acc = acc + scale * part.astype(F32)
            acc = acc * (1.0 / total)
            square = jnp.sum(acc * acc, axis=0, keepdims=True) * (1.0 / HEAD)
            heads.append(acc * lax.rsqrt(square + NORM_EPS))
        return jnp.concatenate(heads, axis=0)

    mixed = jnp.concatenate([joined(0), joined(1)], axis=0)
    mixin[:, :WIDE] = (jnp.transpose(mixed) * fgain_ref[...]).astype(BF16)

    for d in range(1, nf):
        slot = lax.rem(x + d, nf)
        for part in range(2):
            piece = wbuf.at[slot, pl.ds(part * WIDE, WIDE)]
            to_peer(piece, piece, wsend.at[d, part], wrecv.at[part, slot], "fs", slot).wait_recv()
    half = TOK // 2
    columns = wf_ref.shape[1]
    partner = 1 - core
    theirs = mixin[pl.ds(pl.multiple_of(partner * half, half), half), :]
    for slot in range(nf):
        at = slice(slot * columns, (slot + 1) * columns)
        psend[:, at] = dot(theirs, wbuf[slot]).astype(BF16)
    swap = to_peer(psend, precv, psem.at[0], psem.at[1], "tp", partner)
    swap.start()
    mine = mixin[pl.ds(pl.multiple_of(core * half, half), half), :]
    for slot in range(nf):
        at = slice(slot * columns, (slot + 1) * columns)
        out_ref[:, at] = dot(mine, wbuf[slot]).astype(BF16)
    swap.wait()
    out_ref[...] = (out_ref[...].astype(F32) + precv[...].astype(F32)).astype(BF16)

    for ring in rings:
        ring.drain()
    for d in range(1, nf):
        for copy in weight_copies(d):
            copy.wait_send()
    for d in range(1, n1):
        handler_copy(d).wait_send()
        entry_copy(d).wait_send()

    def column_left(d, _):
        column_copy(d).wait_send()
        return 0

    lax.fori_loop(1, n0 - z, column_left, 0)
    for group, size in ((0, n1), (1, n0)):
        for d in range(1, size):
            output_copy(group, d).wait_send()


def solution(mesh):
    nf, n_tp = mesh.shape["fs"], mesh.shape["tp"]
    n0 = 8 if mesh.shape["sp"] == 64 else mesh.shape["sp"] // 2
    n1 = mesh.shape["sp"] // n0
    finer = Mesh(mesh.devices.reshape(n0, n1, nf, n_tp), ("sp_0", "sp_1", "fs", "tp"))

    def shards(q, k, v, f, fgain, r, lk, lv, ll, dl, lgain, wf, wl):
        width = wf.shape[1] * nf
        vm = pl.BlockSpec(memory_space=pltpu.VMEM)
        dma = pltpu.SemaphoreType.DMA
        wide32 = pltpu.VMEM((TOK, WIDE), F32)
        most = max(n0, n1)
        part = (2, most, 2 * HEAD + 16, TOK)
        out = pl.pallas_call(
            functools.partial(kernel, (n0, n1, nf)),
            out_shape=jax.ShapeDtypeStruct((TOK // 2, width), BF16),
            in_specs=[vm] * 13,
            out_specs=vm,
            scratch_shapes=[
                pltpu.VMEM((2, most, PACK, 128), BF16),
                pltpu.VMEM((nf, 2 * WIDE, wf.shape[1]), BF16),
                pltpu.VMEM((2, most, 2 * TOK, 128), BF16),
                pltpu.VMEM((2, most, HEAD, 2 * TOK), F32),
                pltpu.VMEM((2, most, 8, 2 * TOK), F32),
                pltpu.VMEM(part, BF16),
                pltpu.VMEM(part, BF16),
                pltpu.VMEM((n1, 96, 128), BF16),
                pltpu.VMEM((n1, 96, 128), BF16),
                pltpu.VMEM((n0, 96, 128), BF16),
                pltpu.VMEM((n1, 16, 128), BF16),
                pltpu.VMEM((n1, 16, 128), BF16),
                pltpu.VMEM((TOK // 2, width), BF16),
                pltpu.VMEM((TOK // 2, width), BF16),
                pltpu.VMEM((TOK, 2 * WIDE), BF16),
                pltpu.VMEM((TOK, WIDE), BF16),
                wide32,
                wide32,
                wide32,
                wide32,
                wide32,
                wide32,
                wide32,
                wide32,
                pltpu.VMEM((n1, 88, 128), F32),
                dma((2, 2, n1 // 2 + 1)),
                dma((2, n1)),
                dma((2, 2, n0 // 2 + 1)),
                dma((2, n0)),
                dma((nf, 2)),
                dma((2, nf)),
                dma((2, most)),
                dma((2, most)),
                dma((n1,)),
                dma((n1,)),
                dma((n0,)),
                dma((n0,)),
                dma((n1,)),
                dma((n1,)),
                dma((2,)),
            ],
            compiler_params=pltpu.CompilerParams(
                collective_id=0, has_side_effects=True, vmem_limit_bytes=60 * 1024 * 1024
            ),
        )(
            q[0], k[0], v[0], f[0].T, fgain[None], r[0], lk[0], lv[0], ll[0], dl[0], lgain[None], wf, wl
        )
        return out[None]

    heads = P("fs", SP, "tp")
    gains, weights = P("tp"), P("tp", "fs")
    placed = (heads,) * 4 + (gains,) + (heads,) * 5 + (gains, weights, weights)
    return jax.shard_map(
        shards, mesh=finer, in_specs=placed, out_specs=P("fs", SP_TP, None), check_vma=False
    )
```

```python
import functools

import jax
import jax.numpy as jnp
from jax import lax
from jax.experimental import pallas as pl
from jax.experimental.pallas import tpu as pltpu
from jax.sharding import Mesh
from jax.sharding import PartitionSpec as P

HEAD = 64
SPAN = 64
TOK = 256
HEADS = 4
WIDE = HEADS * HEAD
PACK = 640
CHUNK = PACK // 2
SP = ("sp_0", "sp_1")
SP_TP = ("sp_0", "sp_1", "tp")
NORM_EPS = 1e-06
LOW = -1e30
MESH = pl.DeviceIdType.MESH
F32 = jnp.float32
BF16 = jnp.bfloat16


def dot(a, b):
    return lax.dot_general(a, b, (((1,), (0,)), ((), ())), preferred_element_type=F32)


def dot_t(a, b):
    return lax.dot_general(a, b, (((1,), (1,)), ((), ())), preferred_element_type=F32)


def t_dot(a, b):
    return lax.dot_general(a, b, (((0,), (0,)), ((), ())), preferred_element_type=F32)


def iota(shape, dim):
    return lax.broadcasted_iota(jnp.int32, shape, dim)


def three_parts(x):
    high = x.astype(BF16).astype(F32)
    middle = (x - high).astype(BF16).astype(F32)
    return high, middle, x - high - middle


class Ring:
    def __init__(self, axis, size, buf, send, recv):
        self.axis, self.size, self.buf, self.send, self.recv = axis, size, buf, send, recv
        self.me = lax.axis_index(axis)

    def last(self, way, part):
        return self.size // 2 if way == part else (self.size - 1) // 2

    def origin(self, way, step):
        if way == 0:
            return lax.rem(self.me - step + self.size, self.size)
        return lax.rem(self.me + step, self.size)

    def copy(self, way, part, step):
        slot = self.origin(way, step - 1)
        piece = self.buf.at[slot, pl.ds(part * CHUNK, CHUNK)]
        to = lax.rem(self.me + (1 if way == 0 else self.size - 1), self.size)
        return pltpu.make_async_remote_copy(
            src_ref=piece,
            dst_ref=piece,
            send_sem=self.send.at[way, part, step],
            recv_sem=self.recv.at[part, slot],
            device_id={self.axis: to},
            device_id_type=MESH,
        )

    def arrived(self, way, part, step):
        slot = self.origin(way, step)
        piece = self.buf.at[slot, pl.ds(part * CHUNK, CHUNK)]
        pltpu.make_async_remote_copy(
            src_ref=piece,
            dst_ref=piece,
            send_sem=self.send.at[way, part, step],
            recv_sem=self.recv.at[part, slot],
            device_id={self.axis: self.origin(way, 1)},
            device_id_type=MESH,
        ).wait_recv()

    def hop(self, step, part):
        for way in range(2):
            if 1 < step <= self.last(way, part) + 1:
                self.arrived(way, part, step - 1)
            if step <= self.last(way, part):
                self.copy(way, part, step).start()

    def drain(self):
        for part in range(2):
            for way in range(2):
                for step in range(1, self.last(way, part) + 1):
                    self.copy(way, part, step).wait_send()


def to_peer(src, dst, send, recv, axis, to):
    return pltpu.make_async_remote_copy(
        src_ref=src,
        dst_ref=dst,
        send_sem=send,
        recv_sem=recv,
        device_id={axis: to},
        device_id_type=MESH,
    )


def kernel(
    sizes,
    q_ref,
    k_ref,
    v_ref,
    f_ref,
    fgain_ref,
    r_ref,
    lk_ref,
    lv_ref,
    ll_ref,
    dl_ref,
    lgain_ref,
    wf_ref,
    wl_ref,
    out_ref,
    both,
    wbuf,
    pairs,
    accs,
    tops,
    osend,
    okeep,
    hsend,
    hkeep,
    zkeep,
    esend,
    ekeep,
    psend,
    precv,
    mixin,
    ein,
    rin,
    eout,
    wout,
    grown,
    g_s,
    h_s,
    p_s,
    o_s,
    inside,
    ysend,
    yrecv,
    zsend,
    zrecv,
    wsend,
    wrecv,
    osem_send,
    osem_recv,
    hsem_send,
    hsem_recv,
    zsem_send,
    zsem_recv,
    esem_send,
    esem_recv,
    psem,
):
    n0, n1, nf = sizes
    z, y = lax.axis_index("sp_0"), lax.axis_index("sp_1")
    x, core = lax.axis_index("fs"), lax.axis_index("tp")
    lane128 = iota((TOK, 128), 1)

    low_lane = lane128 < HEAD
    ybuf, zbuf = both.at[0], both.at[1]

    def key_block(pair):
        keys = k_ref[...].astype(F32)
        if pair == 1:
            keys = pltpu.roll(keys, HEAD, 1)
        place = iota((128, TOK), 0)
        gates = jnp.zeros((128, TOK), F32)
        for member in range(2):
            line = -f_ref[2 * pair + member : 2 * pair + member + 1, :]
            for k, piece in enumerate(three_parts(line)):
                gates = jnp.where(place == HEAD + 3 * member + k, piece, gates)
        return jnp.where(low_lane, keys, jnp.transpose(gates)).astype(BF16)

    values_t = jnp.transpose(v_ref[...].astype(F32)).astype(BF16)
    queries = (q_ref[...].astype(F32) * 0.125).astype(BF16)
    ybuf[y, 0:TOK] = queries[:, :128]
    zbuf[z, 0:TOK] = queries[:, 128:]
    for pair, buf, slot in ((0, zbuf, z), (1, ybuf, y)):
        buf[slot, TOK : 2 * TOK] = key_block(pair)
        rows = slice(pair * HEAD, (pair + 1) * HEAD)
        buf[slot, 2 * TOK : 2 * TOK + HEAD] = values_t[rows, :128]
        buf[slot, 2 * TOK + HEAD : PACK] = values_t[rows, 128:]

    barrier = pltpu.get_barrier_semaphore()
    peers = [("sp_0", n0, z), ("sp_1", n1, y), ("fs", nf, x), ("tp", 2, core)]
    for axis, size, me in peers:
        for d in range(1, size):
            pl.semaphore_signal(
                barrier, inc=1, device_id={axis: lax.rem(me + d, size)}, device_id_type=MESH
            )
    pl.semaphore_wait(barrier, sum(size - 1 for _, size, _ in peers))

    rings = (Ring("sp_1", n1, ybuf, ysend, yrecv), Ring("sp_0", n0, zbuf, zsend, zrecv))

    def hop(step):
        for part in range(2):
            for ring in rings:
                ring.hop(step, part)

    hop(1)

    def weight_copies(d):
        to = lax.rem(x + d, nf)
        return [
            to_peer(
                ref,
                wbuf.at[x, pl.ds(part * WIDE, WIDE)],
                wsend.at[d, part],
                wrecv.at[part, x],
                "fs",
                to,
            )
            for part, ref in enumerate((wf_ref, wl_ref))
        ]

    row, col = iota((TOK, TOK), 0), iota((TOK, TOK), 1)
    same_span = (row // SPAN) == (col // SPAN)
    same_head = same_span
    strict = jnp.logical_and(same_span, row > col)
    lower = jnp.logical_and(same_span, row >= col)
    head_ones = same_head.astype(F32).astype(BF16)

    def head_sum(t):
        high = t.astype(BF16)
        rest = (t - high.astype(F32)).astype(BF16)
        return dot(high, head_ones) + dot(rest, head_ones)

    lkeys = lk_ref[...].astype(F32)
    unit = lkeys * lax.rsqrt(head_sum(lkeys * lkeys) + NORM_EPS)
    fall = -jnp.exp(dl_ref[...])
    lower_ones = lower.astype(F32).astype(BF16)
    inclusive = sum(dot(lower_ones, piece.astype(BF16)) for piece in three_parts(fall))
    grow = jnp.exp(inclusive)
    shrink = jnp.exp(-inclusive)
    grown[...] = grow
    ein[...] = (-unit * jnp.exp(inclusive - fall)).astype(BF16)
    rin[...] = r_ref[...].astype(F32) * grow
    eout[...] = unit * jax.nn.sigmoid(ll_ref[...].astype(F32)) * shrink
    wout[...] = lkeys * shrink

    for head in range(HEADS):
        in_head = (iota((TOK, WIDE), 1) // HEAD) == head

        def of_head(t):
            return jnp.where(in_head, t.astype(F32), 0.0).astype(BF16)

        e_in = ein[...]
        r_in = rin[...].astype(BF16)
        e_out = of_head(eout[...])
        w_out = of_head(wout[...])
        vals = of_head(lv_ref[...])
        mix_erase = jnp.where(strict, dot_t(e_in, e_out), 0.0)
        mix_write = jnp.where(strict, dot_t(e_in, w_out), 0.0).astype(BF16)
        read_erase = jnp.where(lower, dot_t(r_in, e_out), 0.0).astype(BF16)
        read_write = jnp.where(lower, dot_t(r_in, w_out), 0.0).astype(BF16)

        def level(size):
            odd = jnp.logical_and((row // size) % 2 == 1, (col // size) == (row // size) - 1)
            return jnp.where(odd, mix_erase, 0.0)

        inverse = jnp.where(row == col, 1.0, level(1))
        for size in (2, 4, 8, 16, 32):
            rounded = inverse.astype(BF16)
            step = dot(level(size).astype(BF16), rounded).astype(BF16)
            inverse = inverse + dot(rounded, step)
        inverse = inverse.astype(BF16)
        g_h = dot(inverse, of_head(e_in))
        h_h = dot(inverse, dot(mix_write, vals).astype(BF16))
        p_h = dot(read_erase, g_h.astype(BF16))
        o_h = dot(read_erase, h_h.astype(BF16)) + dot(read_write, vals)
        if head == 0:
            g_s[...], h_s[...], p_s[...], o_s[...] = g_h, h_h, rin[...] + p_h, o_h
        else:
            g_s[...] += g_h
            h_s[...] += h_h
            p_s[...] += p_h
            o_s[...] += o_h
        if head == 1:
            hop(2)

    def compact(t):
        return t[0:64] + t[64:128] + t[128:192] + t[192:256]

    def expand(t):
        copies = t.shape[1] // HEAD
        wide = jnp.concatenate([t.astype(F32)] * copies, axis=0)
        return jnp.where(same_head[: wide.shape[0], : wide.shape[1]], wide, 0.0).astype(BF16)

    def after(earlier, decay, change, added):
        before_decay, before = earlier
        width, rows = before.shape[1], added.shape[0]
        diagonal = iota((64, width), 0) == iota((64, width), 1) % HEAD
        left = before + jnp.concatenate(
            [jnp.where(diagonal, before_decay, 0.0), jnp.zeros((rows, width), F32)], axis=0
        )
        grown_by = jnp.concatenate([jnp.zeros((64, width), F32), added], axis=0)
        return before_decay * decay, before * decay + dot(left.astype(BF16), change) + grown_by

    def decay_rows(decay):
        place = iota((16, decay.shape[1]), 0)
        tail = jnp.zeros((16, decay.shape[1]), F32)
        for k, piece in enumerate(three_parts(decay)):
            tail = jnp.where(place == k, piece, tail)
        return tail.astype(BF16)

    def get_map(t):
        tail = t[80:96].astype(F32)
        return tail[0:1] + tail[1:2] + tail[2:3], t[0:64], t[64:80].astype(F32)

    for span in range(TOK // SPAN):
        at = slice(span * SPAN, (span + 1) * SPAN)
        final = grown[at.stop - 1 : at.stop, :]
        e_f = (eout[at, :] * final).astype(BF16)
        w_f = (wout[at, :] * final).astype(BF16)
        change = jnp.where(same_head, t_dot(g_s[at, :].astype(BF16), e_f), 0.0)
        added = t_dot(h_s[at, :].astype(BF16), e_f) + t_dot(lv_ref[at, :], w_f)
        added = compact(jnp.where(same_head, added, 0.0))
        if span == 0:
            chain = (final, jnp.concatenate([compact(change), added], axis=0))
        else:
            p_span = p_s[at, :].astype(BF16)
            o_s[at, :] += dot_t(p_span, expand(chain[1][64:128]))
            p_s[at, :] = p_s[at, :] * chain[0] + dot_t(p_span, expand(chain[1][0:64]))
            chain = after(chain, final, change.astype(BF16), added)
    for u in range(n1):
        lanes, rows = slice((u // 4) * 128, (u // 4 + 1) * 128), 64 + 16 * (u % 4)
        hsend[u, 0:64] = chain[1][0:64, lanes].astype(BF16)
        hsend[u, 64:80] = chain[1][rows : rows + 16, lanes].astype(BF16)
        hsend[u, 80:96] = decay_rows(chain[0][:, lanes])
    hkeep[y] = hsend[y]

    def handler_copy(d):
        to = lax.rem(y + d, n1)
        return to_peer(
            hsend.at[to], hkeep.at[y], hsem_send.at[d], hsem_recv.at[y], "sp_1", to
        )

    def entry_copy(d):
        to = lax.rem(y + d, n1)
        return to_peer(
            esend.at[to], ekeep.at[y], esem_send.at[d], esem_recv.at[y], "sp_1", to
        )

    def column_copy(d):
        to = lax.rem(z + d, n0)
        return to_peer(zkeep.at[z], zkeep.at[z], zsem_send.at[d], zsem_recv.at[z], "sp_0", to)

    def from_row(keep, send, recv):
        def one(d, _):
            slot = lax.rem(y + d, n1)
            to_peer(keep.at[slot], keep.at[slot], send.at[d], recv.at[slot], "sp_1", slot).wait_recv()
            return 0

        lax.fori_loop(1, n1, one, 0)

    def states_row():
        from_row(hkeep, hsem_send, hsem_recv)
        decay, change, added = get_map(hkeep[0])
        first = (decay, jnp.concatenate([change.astype(F32), added], axis=0))

        def follow(k, so_far):
            inside[k, 0:80] = so_far[1]
            inside[k, 80:88] = jnp.broadcast_to(so_far[0], (8, 128))
            decay, change, added = get_map(hkeep[k])
            return after(so_far, decay, expand(change), added)

        decay, whole = lax.fori_loop(1, n1, follow, first)
        zkeep[z, 0:80] = whole.astype(BF16)
        zkeep[z, 80:96] = decay_rows(decay)

        def send(d, _):
            column_copy(d).start()
            return 0

        lax.fori_loop(1, n0 - z, send, 0)

    def states_column():
        def arrived(slot, _):
            to_peer(
                zkeep.at[slot], zkeep.at[slot], zsem_send.at[0], zsem_recv.at[slot], "sp_0", slot
            ).wait_recv()
            return 0

        lax.fori_loop(0, z, arrived, 0)

        def enter(k, state):
            decay, change, added = get_map(zkeep[k])
            return state * decay + dot(state.astype(BF16), expand(change)) + added

        entry = lax.fori_loop(0, z, enter, jnp.zeros((16, 128), F32))
        esend[0] = entry.astype(BF16)
        for k in range(1, n1):
            here = inside[k]
            moved = entry * here[80:81] + dot(entry.astype(BF16), expand(here[0:64]))
            esend[k] = (moved + here[64:80]).astype(BF16)
        ekeep[y] = esend[y]
        for d in range(1, n1):
            entry_copy(d).start()

    for d in range(1, n1):
        handler_copy(d).start()
    hop(3)
    for d in range(1, nf):
        for copy in weight_copies(d):
            copy.start()
    wbuf[x, 0:WIDE] = wf_ref[...]
    wbuf[x, WIDE : 2 * WIDE] = wl_ref[...]

    def query_pair(raw):
        wide = raw.astype(F32)
        ones = [
            jnp.where(
                jnp.logical_and(lane128 >= HEAD + 3 * m, lane128 < HEAD + 3 * m + 3), 1.0, 0.0
            )
            for m in range(2)
        ]
        first = jnp.where(low_lane, wide, ones[0])
        second = jnp.where(low_lane, pltpu.roll(wide, HEAD, 1), ones[1])
        return jnp.concatenate([first, second], axis=0).astype(BF16)

    def scores_of(q_pair, buf, slots):
        keys = [buf[slot, TOK : 2 * TOK] for slot in slots]
        return dot_t(jnp.concatenate(keys, axis=0) if len(keys) > 1 else keys[0], q_pair)

    def values_of(buf, slots):
        return jnp.concatenate(
            [
                buf[slot, 2 * TOK + part * HEAD : 2 * TOK + (part + 1) * HEAD]
                for slot in slots
                for part in range(2)
            ],
            axis=1,
        )

    def absorb(scores, vals, carry):
        top, total, acc = carry
        new_top = jnp.maximum(top, jnp.max(scores, axis=0, keepdims=True))
        scale = jnp.exp(top - new_top)
        weights = jnp.exp(scores - new_top)
        total = total * scale + jnp.sum(weights, axis=0, keepdims=True)
        return new_top, total, acc * scale + dot(vals, weights.astype(BF16))

    def load(group, block):
        return tops[group, block, 0:1], tops[group, block, 1:2], accs[group, block]

    def save(group, block, carry):
        tops[group, block, 0:1], tops[group, block, 1:2], accs[group, block] = carry

    def put(ref, group, slot, carry):
        top, total, acc = carry
        place = iota((16, TOK), 0)
        tail = jnp.zeros((16, TOK), F32)
        for which, line in enumerate((top, total)):
            for k, piece in enumerate(three_parts(line)):
                for member in range(2):
                    part = piece[:, member * TOK : (member + 1) * TOK]
                    tail = jnp.where(place == 6 * which + 3 * member + k, part, tail)
        acc = acc.astype(BF16)
        ref[group, slot, 0:HEAD] = acc[:, :TOK]
        ref[group, slot, HEAD : 2 * HEAD] = acc[:, TOK:]
        ref[group, slot, 2 * HEAD : 2 * HEAD + 16] = tail.astype(BF16)

    tops[:, :, 0:1] = jnp.full((2, tops.shape[1], 1, 2 * TOK), LOW, F32)
    tops[:, :, 1:2] = jnp.zeros((2, tops.shape[1], 1, 2 * TOK), F32)
    accs[...] = jnp.zeros(accs.shape, F32)
    reach0 = reach1 = min(2, (n0 - 1) // 2, (n1 - 1) // 2)
    row_of, column_of = ("sp_1", n1, y, reach1), ("sp_0", n0, z, reach0)

    def make_pairs(group, first, count):
        axis, size, me, reach = (row_of, column_of)[group]

        def one(d, _):
            block = lax.rem(me + (first % size) + d, size)
            pairs[group, block] = query_pair(both[group, block, 0:TOK])
            return 0

        lax.fori_loop(0, count, one, 0)

    def near(radius):
        side = 2 * radius

        def one(k, _):
            picked = []
            for down, right in ((0, k), (k, side), (side, side - k), (side - k, 0)):
                i = lax.rem(z + down + (n0 - radius), n0)
                j = lax.rem(y + right + (n1 - radius), n1)
                first = jnp.logical_or(i < z, jnp.logical_and(i == z, y < j))
                group = jnp.where(first, 0, 1)
                block, slot = jnp.where(first, j, i), jnp.where(first, i, j)
                buf = both.at[1 - group]
                picked.append((group, block, buf, slot, scores_of(pairs[group, block], buf, [slot])))
            for group, block, buf, slot, scores in picked:
                save(group, block, absorb(scores, values_of(buf, [slot]), load(group, block)))
            return 0

        lax.fori_loop(0, side, one, 0)

    make_pairs(0, -reach1, 2 * reach1 + 1)
    make_pairs(1, -reach0, 2 * reach0 + 1)
    for group, me, slot in ((0, y, z), (1, z, y)):
        carry = load(group, me)
        buf = both.at[1 - group]
        allowed = iota((TOK, 2 * TOK), 0) <= iota((TOK, 2 * TOK), 1) % TOK
        scores = jnp.where(allowed, scores_of(pairs[group, me], buf, [slot]), LOW)
        save(group, me, absorb(scores, values_of(buf, [slot]), carry))
    if reach0 > 0:
        near(1)
    hop(4)
    if reach0 > 1:
        near(2)
    states_row()
    hop(5)
    make_pairs(0, reach1 + 1, n1 - 2 * reach1 - 1)
    make_pairs(1, reach0 + 1, n0 - 2 * reach0 - 1)

    def rest(group, d):
        rows = group == 0
        block = lax.rem(jnp.where(rows, y, z) + d, jnp.where(rows, n1, n0))
        mine, count = jnp.where(rows, z, y), jnp.where(rows, n0, n1)
        is_near = jnp.logical_or(d <= reach0, d >= jnp.where(rows, n1, n0) - reach0)
        start_a = jnp.maximum(jnp.where(is_near, reach0 + 1, 1), n0 - z)
        end_a = jnp.where(is_near, n0 - reach0, n0 + jnp.where(y < block, 1, 0))
        start_b = jnp.where(is_near, reach1 + 1, 0)
        start_b = jnp.where(d == 0, jnp.maximum(start_b, n1 - y), start_b)
        end_b = jnp.where(is_near, n1 - reach1, n1)
        end_b = jnp.where(jnp.logical_and(d > 0, block < z), start_b, end_b)
        start = jnp.where(rows, start_a, start_b)
        length = jnp.maximum(jnp.where(rows, end_a, end_b) - start, 0)
        buf = both.at[1 - group]

        def step(size):
            def one(at, carry):
                slots = [lax.rem(mine + at + k, count) for k in range(size)]
                scores = scores_of(pairs[group, block], buf, slots)
                return absorb(scores, values_of(buf, slots), carry)

            return one

        fours = length // 4
        carry = lax.fori_loop(
            0, fours, lambda k, carry: step(4)(start + 4 * k, carry), load(group, block)
        )
        at = start + 4 * fours
        twos = (length - 4 * fours) // 2
        carry = lax.fori_loop(0, twos, lambda k, carry: step(2)(at + 2 * k, carry), carry)
        at = at + 2 * twos
        return lax.fori_loop(
            0, start + length - at, lambda k, carry: step(1)(at + k, carry), carry
        )

    def output_copy(group, d):
        rows = group == 0
        me = jnp.where(rows, y, z)
        to = lax.rem(me + d, jnp.where(rows, n1, n0))
        return pltpu.make_async_remote_copy(
            src_ref=osend.at[group, d],
            dst_ref=okeep.at[group, me],
            send_sem=osem_send.at[group, d],
            recv_sem=osem_recv.at[group, me],
            device_id={"sp_0": jnp.where(rows, z, to), "sp_1": jnp.where(rows, to, y)},
            device_id_type=MESH,
        )

    def finish(low, high):
        def one(t, _):
            group, d = t % 2, low + t // 2

            @pl.when(d < jnp.where(group == 0, n1, n0))
            def _():
                put(osend, group, d, rest(group, d))
                output_copy(group, d).start()

            return 0

        lax.fori_loop(0, 2 * (high - low), one, 0)

    longest = max(n0, n1)
    finish(1, min(4, longest))
    states_column()
    finish(min(4, longest), longest)

    def own(group, _):
        put(okeep, group, jnp.where(group == 0, y, z), rest(group, 0))
        return 0

    lax.fori_loop(0, 2, own, 0)

    from_row(ekeep, esem_send, esem_recv)
    entry = jnp.concatenate(
        [
            jnp.concatenate([ekeep[4 * tile_of + k] for k in range(4)], axis=0)
            for tile_of in range(2)
        ],
        axis=1,
    )
    read = o_s[...] + dot_t(p_s[...].astype(BF16), expand(entry))
    centred = read - head_sum(read) * (1.0 / HEAD)
    normed = centred * lax.rsqrt(head_sum(centred * centred) * (1.0 / HEAD) + HEAD * 1e-05)
    mixin[:, WIDE:] = (normed * lgain_ref[...]).astype(BF16)

    def joined(group):
        axis, size, me, reach = (row_of, column_of)[group]

        def wait(d, _):
            slot = lax.rem(me + d, size)
            piece = okeep.at[group, slot]
            to_peer(
                piece, piece, osem_send.at[group, d], osem_recv.at[group, slot], axis, slot
            ).wait_recv()
            return 0

        lax.fori_loop(1, size, wait, 0)
        lines = []
        for slot in range(size):
            tail = okeep[group, slot, 2 * HEAD : 2 * HEAD + 16].astype(F32)
            lines.append([tail[3 * k : 3 * k + 1] + tail[3 * k + 1 : 3 * k + 2] + tail[3 * k + 2 : 3 * k + 3] for k in range(4)])
        heads = []
        for member in range(2):
            top = functools.reduce(jnp.maximum, [line[member] for line in lines])
            total, acc = 0.0, 0.0
            for slot in range(size):
                scale = jnp.exp(lines[slot][member] - top)
                total = total + scale * lines[slot][2 + member]
                part = okeep[group, slot, member * HEAD : (member + 1) * HEAD]
                acc = acc + scale * part.astype(F32)
            acc = acc * (1.0 / total)
            square = jnp.sum(acc * acc, axis=0, keepdims=True) * (1.0 / HEAD)
            heads.append(acc * lax.rsqrt(square + NORM_EPS))
        return jnp.concatenate(heads, axis=0)

    mixed = jnp.concatenate([joined(0), joined(1)], axis=0)
    mixin[:, :WIDE] = (jnp.transpose(mixed) * fgain_ref[...]).astype(BF16)

    for d in range(1, nf):
        slot = lax.rem(x + d, nf)
        for part in range(2):
            piece = wbuf.at[slot, pl.ds(part * WIDE, WIDE)]
            to_peer(piece, piece, wsend.at[d, part], wrecv.at[part, slot], "fs", slot).wait_recv()
    half = TOK // 2
    columns = wf_ref.shape[1]
    partner = 1 - core
    theirs = mixin[pl.ds(pl.multiple_of(partner * half, half), half), :]
    for slot in range(nf):
        at = slice(slot * columns, (slot + 1) * columns)
        psend[:, at] = dot(theirs, wbuf[slot]).astype(BF16)
    swap = to_peer(psend, precv, psem.at[0], psem.at[1], "tp", partner)
    swap.start()
    mine = mixin[pl.ds(pl.multiple_of(core * half, half), half), :]
    for slot in range(nf):
        at = slice(slot * columns, (slot + 1) * columns)
        out_ref[:, at] = dot(mine, wbuf[slot]).astype(BF16)
    swap.wait()
    out_ref[...] = (out_ref[...].astype(F32) + precv[...].astype(F32)).astype(BF16)

    for ring in rings:
        ring.drain()
    for d in range(1, nf):
        for copy in weight_copies(d):
            copy.wait_send()
    for d in range(1, n1):
        handler_copy(d).wait_send()
        entry_copy(d).wait_send()

    def column_left(d, _):
        column_copy(d).wait_send()
        return 0

    lax.fori_loop(1, n0 - z, column_left, 0)
    for group, size in ((0, n1), (1, n0)):
        for d in range(1, size):
            output_copy(group, d).wait_send()


def solution(mesh):
    nf, n_tp = mesh.shape["fs"], mesh.shape["tp"]
    n0 = 8 if mesh.shape["sp"] == 64 else mesh.shape["sp"] // 2
    n1 = mesh.shape["sp"] // n0
    finer = Mesh(mesh.devices.reshape(n0, n1, nf, n_tp), ("sp_0", "sp_1", "fs", "tp"))

    def shards(q, k, v, f, fgain, r, lk, lv, ll, dl, lgain, wf, wl):
        width = wf.shape[1] * nf
        vm = pl.BlockSpec(memory_space=pltpu.VMEM)
        dma = pltpu.SemaphoreType.DMA
        wide32 = pltpu.VMEM((TOK, WIDE), F32)
        most = max(n0, n1)
        part = (2, most, 2 * HEAD + 16, TOK)
        out = pl.pallas_call(
            functools.partial(kernel, (n0, n1, nf)),
            out_shape=jax.ShapeDtypeStruct((TOK // 2, width), BF16),
            in_specs=[vm] * 13,
            out_specs=vm,
            scratch_shapes=[
                pltpu.VMEM((2, most, PACK, 128), BF16),
                pltpu.VMEM((nf, 2 * WIDE, wf.shape[1]), BF16),
                pltpu.VMEM((2, most, 2 * TOK, 128), BF16),
                pltpu.VMEM((2, most, HEAD, 2 * TOK), F32),
                pltpu.VMEM((2, most, 8, 2 * TOK), F32),
                pltpu.VMEM(part, BF16),
                pltpu.VMEM(part, BF16),
                pltpu.VMEM((n1, 96, 128), BF16),
                pltpu.VMEM((n1, 96, 128), BF16),
                pltpu.VMEM((n0, 96, 128), BF16),
                pltpu.VMEM((n1, 16, 128), BF16),
                pltpu.VMEM((n1, 16, 128), BF16),
                pltpu.VMEM((TOK // 2, width), BF16),
                pltpu.VMEM((TOK // 2, width), BF16),
                pltpu.VMEM((TOK, 2 * WIDE), BF16),
                pltpu.VMEM((TOK, WIDE), BF16),
                wide32,
                wide32,
                wide32,
                wide32,
                wide32,
                wide32,
                wide32,
                wide32,
                pltpu.VMEM((n1, 88, 128), F32),
                dma((2, 2, n1 // 2 + 1)),
                dma((2, n1)),
                dma((2, 2, n0 // 2 + 1)),
                dma((2, n0)),
                dma((nf, 2)),
                dma((2, nf)),
                dma((2, most)),
                dma((2, most)),
                dma((n1,)),
                dma((n1,)),
                dma((n0,)),
                dma((n0,)),
                dma((n1,)),
                dma((n1,)),
                dma((2,)),
            ],
            compiler_params=pltpu.CompilerParams(
                collective_id=0, has_side_effects=True, vmem_limit_bytes=60 * 1024 * 1024
            ),
        )(
            q[0], k[0], v[0], f[0].T, fgain[None], r[0], lk[0], lv[0], ll[0], dl[0], lgain[None], wf, wl
        )
        return out[None]

    heads = P("fs", SP, "tp")
    gains, weights = P("tp"), P("tp", "fs")
    placed = (heads,) * 4 + (gains,) + (heads,) * 5 + (gains, weights, weights)
    return jax.shard_map(
        shards, mesh=finer, in_specs=placed, out_specs=P("fs", SP_TP, None), check_vma=False
    )
```

```python
import functools

import jax
import jax.numpy as jnp
from jax import lax
from jax.experimental import pallas as pl
from jax.experimental.pallas import tpu as pltpu
from jax.sharding import Mesh
from jax.sharding import PartitionSpec as P

HEAD = 64
SPAN = 64
TOK = 256
HEADS = 4
WIDE = HEADS * HEAD
PACK = 640
CHUNK = PACK // 2
SP = ("sp_0", "sp_1")
SP_TP = ("sp_0", "sp_1", "tp")
NORM_EPS = 1e-06
LOW = -1e30
MESH = pl.DeviceIdType.MESH
F32 = jnp.float32
BF16 = jnp.bfloat16


def dot(a, b):
    return lax.dot_general(a, b, (((1,), (0,)), ((), ())), preferred_element_type=F32)


def dot_t(a, b):
    return lax.dot_general(a, b, (((1,), (1,)), ((), ())), preferred_element_type=F32)


def t_dot(a, b):
    return lax.dot_general(a, b, (((0,), (0,)), ((), ())), preferred_element_type=F32)


def iota(shape, dim):
    return lax.broadcasted_iota(jnp.int32, shape, dim)


def three_parts(x):
    high = x.astype(BF16).astype(F32)
    middle = (x - high).astype(BF16).astype(F32)
    return high, middle, x - high - middle


class Ring:
    def __init__(self, axis, size, buf, send, recv):
        self.axis, self.size, self.buf, self.send, self.recv = axis, size, buf, send, recv
        self.me = lax.axis_index(axis)

    def last(self, way, part):
        return self.size // 2 if way == part else (self.size - 1) // 2

    def origin(self, way, step):
        if way == 0:
            return lax.rem(self.me - step + self.size, self.size)
        return lax.rem(self.me + step, self.size)

    def copy(self, way, part, step):
        slot = self.origin(way, step - 1)
        piece = self.buf.at[slot, pl.ds(part * CHUNK, CHUNK)]
        to = lax.rem(self.me + (1 if way == 0 else self.size - 1), self.size)
        return pltpu.make_async_remote_copy(
            src_ref=piece,
            dst_ref=piece,
            send_sem=self.send.at[way, part, step],
            recv_sem=self.recv.at[part, slot],
            device_id={self.axis: to},
            device_id_type=MESH,
        )

    def arrived(self, way, part, step):
        slot = self.origin(way, step)
        piece = self.buf.at[slot, pl.ds(part * CHUNK, CHUNK)]
        pltpu.make_async_remote_copy(
            src_ref=piece,
            dst_ref=piece,
            send_sem=self.send.at[way, part, step],
            recv_sem=self.recv.at[part, slot],
            device_id={self.axis: self.origin(way, 1)},
            device_id_type=MESH,
        ).wait_recv()

    def hop(self, step, part):
        for way in range(2):
            if 1 < step <= self.last(way, part) + 1:
                self.arrived(way, part, step - 1)
            if step <= self.last(way, part):
                self.copy(way, part, step).start()

    def drain(self):
        for part in range(2):
            for way in range(2):
                for step in range(1, self.last(way, part) + 1):
                    self.copy(way, part, step).wait_send()


def to_peer(src, dst, send, recv, axis, to):
    return pltpu.make_async_remote_copy(
        src_ref=src,
        dst_ref=dst,
        send_sem=send,
        recv_sem=recv,
        device_id={axis: to},
        device_id_type=MESH,
    )


def kernel(
    sizes,
    q_ref,
    k_ref,
    v_ref,
    f_ref,
    fgain_ref,
    r_ref,
    lk_ref,
    lv_ref,
    ll_ref,
    dl_ref,
    lgain_ref,
    wf_ref,
    wl_ref,
    out_ref,
    both,
    wbuf,
    pairs,
    accs,
    tops,
    osend,
    okeep,
    hsend,
    hkeep,
    zkeep,
    esend,
    ekeep,
    psend,
    precv,
    mixin,
    sums,
    ein,
    rin,
    eout,
    wout,
    grown,
    g_s,
    h_s,
    p_s,
    o_s,
    inside,
    ysend,
    yrecv,
    zsend,
    zrecv,
    wsend,
    wrecv,
    osem_send,
    osem_recv,
    hsem_send,
    hsem_recv,
    zsem_send,
    zsem_recv,
    esem_send,
    esem_recv,
    psem,
):
    n0, n1, nf = sizes
    z, y = lax.axis_index("sp_0"), lax.axis_index("sp_1")
    x, core = lax.axis_index("fs"), lax.axis_index("tp")
    lane128 = iota((TOK, 128), 1)

    low_lane = lane128 < HEAD
    ybuf, zbuf = both.at[0], both.at[1]

    def key_block(pair):
        keys = k_ref[...].astype(F32)
        if pair == 1:
            keys = pltpu.roll(keys, HEAD, 1)
        place = iota((128, TOK), 0)
        gates = jnp.zeros((128, TOK), F32)
        for member in range(2):
            line = -f_ref[2 * pair + member : 2 * pair + member + 1, :]
            for k, piece in enumerate(three_parts(line)):
                gates = jnp.where(place == HEAD + 3 * member + k, piece, gates)
        return jnp.where(low_lane, keys, jnp.transpose(gates)).astype(BF16)

    values_t = jnp.transpose(v_ref[...].astype(F32)).astype(BF16)
    queries = (q_ref[...].astype(F32) * 0.125).astype(BF16)
    ybuf[y, 0:TOK] = queries[:, :128]
    zbuf[z, 0:TOK] = queries[:, 128:]
    for pair, buf, slot in ((0, zbuf, z), (1, ybuf, y)):
        buf[slot, TOK : 2 * TOK] = key_block(pair)
        rows = slice(pair * HEAD, (pair + 1) * HEAD)
        buf[slot, 2 * TOK : 2 * TOK + HEAD] = values_t[rows, :128]
        buf[slot, 2 * TOK + HEAD : PACK] = values_t[rows, 128:]

    barrier = pltpu.get_barrier_semaphore()
    peers = [("sp_0", n0, z), ("sp_1", n1, y), ("fs", nf, x), ("tp", 2, core)]
    for axis, size, me in peers:
        for d in range(1, size):
            pl.semaphore_signal(
                barrier, inc=1, device_id={axis: lax.rem(me + d, size)}, device_id_type=MESH
            )
    pl.semaphore_wait(barrier, sum(size - 1 for _, size, _ in peers))

    rings = (Ring("sp_1", n1, ybuf, ysend, yrecv), Ring("sp_0", n0, zbuf, zsend, zrecv))

    def hop(step, part):
        for ring in rings:
            ring.hop(step, part)

    hop(1, 0)
    hop(1, 1)

    def weight_copies(d):
        to = lax.rem(x + d, nf)
        return [
            to_peer(
                ref,
                wbuf.at[x, pl.ds(part * WIDE, WIDE)],
                wsend.at[d, part],
                wrecv.at[part, x],
                "fs",
                to,
            )
            for part, ref in enumerate((wf_ref, wl_ref))
        ]

    row, col = iota((TOK, TOK), 0), iota((TOK, TOK), 1)
    same_span = (row // SPAN) == (col // SPAN)
    same_head = same_span
    strict = jnp.logical_and(same_span, row > col)
    lower = jnp.logical_and(same_span, row >= col)
    head_ones = same_head.astype(F32).astype(BF16)

    def head_sum(t):
        high = t.astype(BF16)
        rest = (t - high.astype(F32)).astype(BF16)
        return dot(high, head_ones) + dot(rest, head_ones)

    lkeys = lk_ref[...].astype(F32)
    unit = lkeys * lax.rsqrt(head_sum(lkeys * lkeys) + NORM_EPS)
    fall = -jnp.exp(dl_ref[...])
    lower_ones = lower.astype(F32).astype(BF16)
    inclusive = sum(dot(lower_ones, piece.astype(BF16)) for piece in three_parts(fall))
    grow = jnp.exp(inclusive)
    shrink = jnp.exp(-inclusive)
    grown[...] = grow
    ein[...] = (-unit * jnp.exp(inclusive - fall)).astype(BF16)
    rin[...] = r_ref[...].astype(F32) * grow
    eout[...] = unit * jax.nn.sigmoid(ll_ref[...].astype(F32)) * shrink
    wout[...] = lkeys * shrink

    for head in range(HEADS):
        in_head = (iota((TOK, WIDE), 1) // HEAD) == head

        def of_head(t):
            return jnp.where(in_head, t.astype(F32), 0.0).astype(BF16)

        e_in = ein[...]
        r_in = rin[...].astype(BF16)
        e_out = of_head(eout[...])
        w_out = of_head(wout[...])
        vals = of_head(lv_ref[...])
        mix_erase = jnp.where(strict, dot_t(e_in, e_out), 0.0)
        mix_write = jnp.where(strict, dot_t(e_in, w_out), 0.0).astype(BF16)
        read_erase = jnp.where(lower, dot_t(r_in, e_out), 0.0).astype(BF16)
        read_write = jnp.where(lower, dot_t(r_in, w_out), 0.0).astype(BF16)

        def level(size):
            odd = jnp.logical_and((row // size) % 2 == 1, (col // size) == (row // size) - 1)
            return jnp.where(odd, mix_erase, 0.0)

        inverse = jnp.where(row == col, 1.0, level(1))
        for size in (2, 4, 8, 16, 32):
            rounded = inverse.astype(BF16)
            step = dot(level(size).astype(BF16), rounded).astype(BF16)
            inverse = inverse + dot(rounded, step)
        inverse = inverse.astype(BF16)
        g_h = dot(inverse, of_head(e_in))
        h_h = dot(inverse, dot(mix_write, vals).astype(BF16))
        p_h = dot(read_erase, g_h.astype(BF16))
        o_h = dot(read_erase, h_h.astype(BF16)) + dot(read_write, vals)
        if head == 0:
            g_s[...], h_s[...], p_s[...], o_s[...] = g_h, h_h, rin[...] + p_h, o_h
        else:
            g_s[...] += g_h
            h_s[...] += h_h
            p_s[...] += p_h
            o_s[...] += o_h
        hop(2 + head // 2, head % 2)

    def compact(t):
        return t[0:64] + t[64:128] + t[128:192] + t[192:256]

    def expand(t):
        copies = t.shape[1] // HEAD
        wide = jnp.concatenate([t.astype(F32)] * copies, axis=0)
        return jnp.where(same_head[: wide.shape[0], : wide.shape[1]], wide, 0.0).astype(BF16)

    def after(earlier, decay, change, added):
        before_decay, before = earlier
        width, rows = before.shape[1], added.shape[0]
        diagonal = iota((64, width), 0) == iota((64, width), 1) % HEAD
        left = before + jnp.concatenate(
            [jnp.where(diagonal, before_decay, 0.0), jnp.zeros((rows, width), F32)], axis=0
        )
        grown_by = jnp.concatenate([jnp.zeros((64, width), F32), added], axis=0)
        return before_decay * decay, before * decay + dot(left.astype(BF16), change) + grown_by

    def decay_rows(decay):
        place = iota((16, decay.shape[1]), 0)
        tail = jnp.zeros((16, decay.shape[1]), F32)
        for k, piece in enumerate(three_parts(decay)):
            tail = jnp.where(place == k, piece, tail)
        return tail.astype(BF16)

    def get_map(t):
        tail = t[80:96].astype(F32)
        return tail[0:1] + tail[1:2] + tail[2:3], t[0:64], t[64:80].astype(F32)

    for span in range(TOK // SPAN):
        at = slice(span * SPAN, (span + 1) * SPAN)
        final = grown[at.stop - 1 : at.stop, :]
        e_f = (eout[at, :] * final).astype(BF16)
        w_f = (wout[at, :] * final).astype(BF16)
        change = jnp.where(same_head, t_dot(g_s[at, :].astype(BF16), e_f), 0.0)
        added = t_dot(h_s[at, :].astype(BF16), e_f) + t_dot(lv_ref[at, :], w_f)
        added = compact(jnp.where(same_head, added, 0.0))
        if span == 0:
            chain = (final, jnp.concatenate([compact(change), added], axis=0))
        else:
            p_span = p_s[at, :].astype(BF16)
            o_s[at, :] += dot_t(p_span, expand(chain[1][64:128]))
            p_s[at, :] = p_s[at, :] * chain[0] + dot_t(p_span, expand(chain[1][0:64]))
            chain = after(chain, final, change.astype(BF16), added)
    for u in range(n1):
        lanes, rows = slice((u // 4) * 128, (u // 4 + 1) * 128), 64 + 16 * (u % 4)
        hsend[u, 0:64] = chain[1][0:64, lanes].astype(BF16)
        hsend[u, 64:80] = chain[1][rows : rows + 16, lanes].astype(BF16)
        hsend[u, 80:96] = decay_rows(chain[0][:, lanes])
    hkeep[y] = hsend[y]

    def handler_copy(d):
        to = lax.rem(y + d, n1)
        return to_peer(
            hsend.at[to], hkeep.at[y], hsem_send.at[d], hsem_recv.at[y], "sp_1", to
        )

    def entry_copy(d):
        to = lax.rem(y + d, n1)
        return to_peer(
            esend.at[to], ekeep.at[y], esem_send.at[d], esem_recv.at[y], "sp_1", to
        )

    def column_copy(d):
        to = lax.rem(z + d, n0)
        return to_peer(zkeep.at[z], zkeep.at[z], zsem_send.at[d], zsem_recv.at[z], "sp_0", to)

    def from_row(keep, send, recv):
        def one(d, _):
            slot = lax.rem(y + d, n1)
            to_peer(keep.at[slot], keep.at[slot], send.at[d], recv.at[slot], "sp_1", slot).wait_recv()
            return 0

        lax.fori_loop(1, n1, one, 0)

    def states_row():
        from_row(hkeep, hsem_send, hsem_recv)
        decay, change, added = get_map(hkeep[0])
        first = (decay, jnp.concatenate([change.astype(F32), added], axis=0))

        def follow(k, so_far):
            inside[k, 0:80] = so_far[1]
            inside[k, 80:88] = jnp.broadcast_to(so_far[0], (8, 128))
            decay, change, added = get_map(hkeep[k])
            return after(so_far, decay, expand(change), added)

        decay, whole = lax.fori_loop(1, n1, follow, first)
        zkeep[z, 0:80] = whole.astype(BF16)
        zkeep[z, 80:96] = decay_rows(decay)

        def send(d, _):
            column_copy(d).start()
            return 0

        lax.fori_loop(1, n0 - z, send, 0)

    def states_column():
        def arrived(slot, _):
            to_peer(
                zkeep.at[slot], zkeep.at[slot], zsem_send.at[0], zsem_recv.at[slot], "sp_0", slot
            ).wait_recv()
            return 0

        lax.fori_loop(0, z, arrived, 0)

        def enter(k, state):
            decay, change, added = get_map(zkeep[k])
            return state * decay + dot(state.astype(BF16), expand(change)) + added

        entry = lax.fori_loop(0, z, enter, jnp.zeros((16, 128), F32))
        esend[0] = entry.astype(BF16)
        for k in range(1, n1):
            here = inside[k]
            moved = entry * here[80:81] + dot(entry.astype(BF16), expand(here[0:64]))
            esend[k] = (moved + here[64:80]).astype(BF16)
        ekeep[y] = esend[y]
        for d in range(1, n1):
            entry_copy(d).start()

    hop(4, 0)
    for d in range(1, n1):
        handler_copy(d).start()
    for d in range(1, nf):
        for copy in weight_copies(d):
            copy.start()
    wbuf[x, 0:WIDE] = wf_ref[...]
    wbuf[x, WIDE : 2 * WIDE] = wl_ref[...]

    def query_pair(raw):
        wide = raw.astype(F32)
        ones = [
            jnp.where(
                jnp.logical_and(lane128 >= HEAD + 3 * m, lane128 < HEAD + 3 * m + 3), 1.0, 0.0
            )
            for m in range(2)
        ]
        first = jnp.where(low_lane, wide, ones[0])
        second = jnp.where(low_lane, pltpu.roll(wide, HEAD, 1), ones[1])
        return jnp.concatenate([first, second], axis=0).astype(BF16)

    def scores_of(q_pair, buf, slots):
        keys = [buf[slot, TOK : 2 * TOK] for slot in slots]
        return dot_t(jnp.concatenate(keys, axis=0) if len(keys) > 1 else keys[0], q_pair)

    def values_of(buf, slots):
        return jnp.concatenate(
            [
                buf[slot, 2 * TOK + part * HEAD : 2 * TOK + (part + 1) * HEAD]
                for slot in slots
                for part in range(2)
            ],
            axis=1,
        )

    def absorb(scores, vals, carry):
        top, total, acc = carry
        new_top = jnp.maximum(top, jnp.max(scores, axis=0, keepdims=True))
        scale = jnp.exp(top - new_top)
        weights = jnp.exp(scores - new_top)
        total = total * scale + jnp.sum(weights, axis=0, keepdims=True)
        return new_top, total, acc * scale + dot(vals, weights.astype(BF16))

    def load(group, block):
        return tops[group, block, 0:1], tops[group, block, 1:2], accs[group, block]

    def save(group, block, carry):
        tops[group, block, 0:1], tops[group, block, 1:2], accs[group, block] = carry

    def put(ref, group, slot, carry):
        top, total, acc = carry
        place = iota((16, TOK), 0)
        tail = jnp.zeros((16, TOK), F32)
        for which, line in enumerate((top, total)):
            for k, piece in enumerate(three_parts(line)):
                for member in range(2):
                    part = piece[:, member * TOK : (member + 1) * TOK]
                    tail = jnp.where(place == 6 * which + 3 * member + k, part, tail)
        acc = acc.astype(BF16)
        ref[group, slot, 0:HEAD] = acc[:, :TOK]
        ref[group, slot, HEAD : 2 * HEAD] = acc[:, TOK:]
        ref[group, slot, 2 * HEAD : 2 * HEAD + 16] = tail.astype(BF16)

    tops[:, :, 0:1] = jnp.full((2, tops.shape[1], 1, 2 * TOK), LOW, F32)
    tops[:, :, 1:2] = jnp.zeros((2, tops.shape[1], 1, 2 * TOK), F32)
    accs[...] = jnp.zeros(accs.shape, F32)
    reach0 = reach1 = min(1, (n0 - 1) // 2, (n1 - 1) // 2)
    row_of, column_of = ("sp_1", n1, y, reach1), ("sp_0", n0, z, reach0)

    def make_pairs(group, first, count):
        axis, size, me, reach = (row_of, column_of)[group]

        def one(d, _):
            block = lax.rem(me + (first % size) + d, size)
            pairs[group, block] = query_pair(both[group, block, 0:TOK])
            return 0

        lax.fori_loop(0, count, one, 0)

    def near(radius):
        side = 2 * radius

        def one(k, _):
            picked = []
            for down, right in ((0, k), (k, side), (side, side - k), (side - k, 0)):
                i = lax.rem(z + down + (n0 - radius), n0)
                j = lax.rem(y + right + (n1 - radius), n1)
                first = jnp.logical_or(i < z, jnp.logical_and(i == z, y < j))
                group = jnp.where(first, 0, 1)
                block, slot = jnp.where(first, j, i), jnp.where(first, i, j)
                buf = both.at[1 - group]
                picked.append((group, block, buf, slot, scores_of(pairs[group, block], buf, [slot])))
            for group, block, buf, slot, scores in picked:
                save(group, block, absorb(scores, values_of(buf, [slot]), load(group, block)))
            return 0

        lax.fori_loop(0, side, one, 0)

    make_pairs(0, -reach1, 2 * reach1 + 1)
    make_pairs(1, -reach0, 2 * reach0 + 1)
    for group, me, slot in ((0, y, z), (1, z, y)):
        carry = load(group, me)
        buf = both.at[1 - group]
        allowed = iota((TOK, 2 * TOK), 0) <= iota((TOK, 2 * TOK), 1) % TOK
        scores = jnp.where(allowed, scores_of(pairs[group, me], buf, [slot]), LOW)
        save(group, me, absorb(scores, values_of(buf, [slot]), carry))
    hop(4, 1)
    if reach0 > 0:
        near(1)
    hop(5, 0)
    hop(5, 1)
    make_pairs(0, reach1 + 1, n1 - 2 * reach1 - 1)
    make_pairs(1, reach0 + 1, n0 - 2 * reach0 - 1)

    def rest(group, d):
        rows = group == 0
        block = lax.rem(jnp.where(rows, y, z) + d, jnp.where(rows, n1, n0))
        mine, count = jnp.where(rows, z, y), jnp.where(rows, n0, n1)
        is_near = jnp.logical_or(d <= reach0, d >= jnp.where(rows, n1, n0) - reach0)
        start_a = jnp.maximum(jnp.where(is_near, reach0 + 1, 1), n0 - z)
        end_a = jnp.where(is_near, n0 - reach0, n0 + jnp.where(y < block, 1, 0))
        start_b = jnp.where(is_near, reach1 + 1, 0)
        start_b = jnp.where(d == 0, jnp.maximum(start_b, n1 - y), start_b)
        end_b = jnp.where(is_near, n1 - reach1, n1)
        end_b = jnp.where(jnp.logical_and(d > 0, block < z), start_b, end_b)
        start = jnp.where(rows, start_a, start_b)
        length = jnp.maximum(jnp.where(rows, end_a, end_b) - start, 0)
        buf = both.at[1 - group]

        def step(size):
            def one(at, carry):
                slots = [lax.rem(mine + at + k, count) for k in range(size)]
                scores = scores_of(pairs[group, block], buf, slots)
                return absorb(scores, values_of(buf, slots), carry)

            return one

        fours = length // 4
        carry = lax.fori_loop(
            0, fours, lambda k, carry: step(4)(start + 4 * k, carry), load(group, block)
        )
        at = start + 4 * fours
        twos = (length - 4 * fours) // 2
        carry = lax.fori_loop(0, twos, lambda k, carry: step(2)(at + 2 * k, carry), carry)
        at = at + 2 * twos
        return lax.fori_loop(
            0, start + length - at, lambda k, carry: step(1)(at + k, carry), carry
        )

    def output_copy(group, d):
        rows = group == 0
        me = jnp.where(rows, y, z)
        to = lax.rem(me + d, jnp.where(rows, n1, n0))
        return pltpu.make_async_remote_copy(
            src_ref=osend.at[group, d],
            dst_ref=okeep.at[group, me],
            send_sem=osem_send.at[group, d],
            recv_sem=osem_recv.at[group, me],
            device_id={"sp_0": jnp.where(rows, z, to), "sp_1": jnp.where(rows, to, y)},
            device_id_type=MESH,
        )

    longest = max(n0, n1)
    row_turn, column_turn = 2 % (2 * longest - 2), min(7, 2 * longest - 3)

    def finish(t, _):
        group, turn = t % 2, t // 2
        d = longest // 2 + jnp.where(turn % 2 == 1, -((turn + 1) // 2), turn // 2)

        @pl.when(t == row_turn)
        def _():
            states_row()

        @pl.when(t == column_turn)
        def _():
            states_column()

        @pl.when(d < jnp.where(group == 0, n1, n0))
        def _():
            put(osend, group, d, rest(group, d))
            output_copy(group, d).start()

        return 0

    lax.fori_loop(0, 2 * (longest - 1), finish, 0)

    def own(group, _):
        put(okeep, group, jnp.where(group == 0, y, z), rest(group, 0))
        return 0

    lax.fori_loop(0, 2, own, 0)

    from_row(ekeep, esem_send, esem_recv)
    entry = jnp.concatenate(
        [
            jnp.concatenate([ekeep[4 * tile_of + k] for k in range(4)], axis=0)
            for tile_of in range(2)
        ],
        axis=1,
    )
    read = o_s[...] + dot_t(p_s[...].astype(BF16), expand(entry))
    centred = read - head_sum(read) * (1.0 / HEAD)
    normed = centred * lax.rsqrt(head_sum(centred * centred) * (1.0 / HEAD) + HEAD * 1e-05)
    mixin[:, WIDE:] = (normed * lgain_ref[...]).astype(BF16)

    for d in range(1, nf):
        slot = lax.rem(x + d, nf)
        for part in range(2):
            piece = wbuf.at[slot, pl.ds(part * WIDE, WIDE)]
            to_peer(piece, piece, wsend.at[d, part], wrecv.at[part, slot], "fs", slot).wait_recv()
    columns = wf_ref.shape[1]
    slices = [slice(slot * columns, (slot + 1) * columns) for slot in range(nf)]
    lin_out = mixin[:, WIDE:]
    for slot, at in enumerate(slices):
        sums[:, at] = dot(lin_out, wbuf[slot, WIDE : 2 * WIDE])

    def joined(group):
        axis, size, me, reach = (row_of, column_of)[group]

        def wait(d, _):
            slot = lax.rem(me + d, size)
            piece = okeep.at[group, slot]
            to_peer(
                piece, piece, osem_send.at[group, d], osem_recv.at[group, slot], axis, slot
            ).wait_recv()
            return 0

        lax.fori_loop(1, size, wait, 0)
        lines = []
        for slot in range(size):
            tail = okeep[group, slot, 2 * HEAD : 2 * HEAD + 16].astype(F32)
            lines.append([tail[3 * k : 3 * k + 1] + tail[3 * k + 1 : 3 * k + 2] + tail[3 * k + 2 : 3 * k + 3] for k in range(4)])
        heads = []
        for member in range(2):
            top = functools.reduce(jnp.maximum, [line[member] for line in lines])
            total, acc = 0.0, 0.0
            for slot in range(size):
                scale = jnp.exp(lines[slot][member] - top)
                total = total + scale * lines[slot][2 + member]
                part = okeep[group, slot, member * HEAD : (member + 1) * HEAD]
                acc = acc + scale * part.astype(F32)
            acc = acc * (1.0 / total)
            square = jnp.sum(acc * acc, axis=0, keepdims=True) * (1.0 / HEAD)
            heads.append(acc * lax.rsqrt(square + NORM_EPS))
        return jnp.concatenate(heads, axis=0)

    mixed = jnp.concatenate([joined(0), joined(1)], axis=0)
    mixin[:, :WIDE] = (jnp.transpose(mixed) * fgain_ref[...]).astype(BF16)

    half = TOK // 2
    partner = 1 - core
    theirs = pl.ds(pl.multiple_of(partner * half, half), half)
    mine = pl.ds(pl.multiple_of(core * half, half), half)
    for slot, at in enumerate(slices):
        added = dot(mixin[theirs, :WIDE], wbuf[slot, 0:WIDE])
        psend[:, at] = (sums[theirs, at] + added).astype(BF16)
    swap = to_peer(psend, precv, psem.at[0], psem.at[1], "tp", partner)
    swap.start()
    for slot, at in enumerate(slices):
        added = dot(mixin[mine, :WIDE], wbuf[slot, 0:WIDE])
        sums[mine, at] = (sums[mine, at] + added).astype(BF16).astype(F32)
    swap.wait()
    out_ref[...] = (sums[mine, :] + precv[...].astype(F32)).astype(BF16)

    for ring in rings:
        ring.drain()
    for d in range(1, nf):
        for copy in weight_copies(d):
            copy.wait_send()
    for d in range(1, n1):
        handler_copy(d).wait_send()
        entry_copy(d).wait_send()

    def column_left(d, _):
        column_copy(d).wait_send()
        return 0

    lax.fori_loop(1, n0 - z, column_left, 0)
    for group, size in ((0, n1), (1, n0)):
        for d in range(1, size):
            output_copy(group, d).wait_send()


def solution(mesh):
    nf, n_tp = mesh.shape["fs"], mesh.shape["tp"]
    n0 = 8 if mesh.shape["sp"] == 64 else mesh.shape["sp"] // 2
    n1 = mesh.shape["sp"] // n0
    finer = Mesh(mesh.devices.reshape(n0, n1, nf, n_tp), ("sp_0", "sp_1", "fs", "tp"))

    def shards(q, k, v, f, fgain, r, lk, lv, ll, dl, lgain, wf, wl):
        width = wf.shape[1] * nf
        vm = pl.BlockSpec(memory_space=pltpu.VMEM)
        dma = pltpu.SemaphoreType.DMA
        wide32 = pltpu.VMEM((TOK, WIDE), F32)
        most = max(n0, n1)
        part = (2, most, 2 * HEAD + 16, TOK)
        out = pl.pallas_call(
            functools.partial(kernel, (n0, n1, nf)),
            out_shape=jax.ShapeDtypeStruct((TOK // 2, width), BF16),
            in_specs=[vm] * 13,
            out_specs=vm,
            scratch_shapes=[
                pltpu.VMEM((2, most, PACK, 128), BF16),
                pltpu.VMEM((nf, 2 * WIDE, wf.shape[1]), BF16),
                pltpu.VMEM((2, most, 2 * TOK, 128), BF16),
                pltpu.VMEM((2, most, HEAD, 2 * TOK), F32),
                pltpu.VMEM((2, most, 8, 2 * TOK), F32),
                pltpu.VMEM(part, BF16),
                pltpu.VMEM(part, BF16),
                pltpu.VMEM((n1, 96, 128), BF16),
                pltpu.VMEM((n1, 96, 128), BF16),
                pltpu.VMEM((n0, 96, 128), BF16),
                pltpu.VMEM((n1, 16, 128), BF16),
                pltpu.VMEM((n1, 16, 128), BF16),
                pltpu.VMEM((TOK // 2, width), BF16),
                pltpu.VMEM((TOK // 2, width), BF16),
                pltpu.VMEM((TOK, 2 * WIDE), BF16),
                pltpu.VMEM((TOK, width), F32),
                pltpu.VMEM((TOK, WIDE), BF16),
                wide32,
                wide32,
                wide32,
                wide32,
                wide32,
                wide32,
                wide32,
                wide32,
                pltpu.VMEM((n1, 88, 128), F32),
                dma((2, 2, n1 // 2 + 1)),
                dma((2, n1)),
                dma((2, 2, n0 // 2 + 1)),
                dma((2, n0)),
                dma((nf, 2)),
                dma((2, nf)),
                dma((2, most)),
                dma((2, most)),
                dma((n1,)),
                dma((n1,)),
                dma((n0,)),
                dma((n0,)),
                dma((n1,)),
                dma((n1,)),
                dma((2,)),
            ],
            compiler_params=pltpu.CompilerParams(
                collective_id=0, has_side_effects=True, vmem_limit_bytes=60 * 1024 * 1024
            ),
        )(
            q[0], k[0], v[0], f[0].T, fgain[None], r[0], lk[0], lv[0], ll[0], dl[0], lgain[None], wf, wl
        )
        return out[None]

    heads = P("fs", SP, "tp")
    gains, weights = P("tp"), P("tp", "fs")
    placed = (heads,) * 4 + (gains,) + (heads,) * 5 + (gains, weights, weights)
    return jax.shard_map(
        shards, mesh=finer, in_specs=placed, out_specs=P("fs", SP_TP, None), check_vma=False
    )
```

```python
import functools

import jax
import jax.numpy as jnp
from jax import lax
from jax.experimental import pallas as pl
from jax.experimental.pallas import tpu as pltpu
from jax.sharding import Mesh
from jax.sharding import PartitionSpec as P

HEAD = 64
SPAN = 64
TOK = 256
HEADS = 4
WIDE = HEADS * HEAD
PACK = 640
CHUNK = PACK // 2
SP = ("sp_0", "sp_1")
SP_TP = ("sp_0", "sp_1", "tp")
NORM_EPS = 1e-06
LOW = -1e30
MESH = pl.DeviceIdType.MESH
F32 = jnp.float32
BF16 = jnp.bfloat16


def dot(a, b):
    return lax.dot_general(a, b, (((1,), (0,)), ((), ())), preferred_element_type=F32)


def dot_t(a, b):
    return lax.dot_general(a, b, (((1,), (1,)), ((), ())), preferred_element_type=F32)


def t_dot(a, b):
    return lax.dot_general(a, b, (((0,), (0,)), ((), ())), preferred_element_type=F32)


def iota(shape, dim):
    return lax.broadcasted_iota(jnp.int32, shape, dim)


def three_parts(x):
    high = x.astype(BF16).astype(F32)
    middle = (x - high).astype(BF16).astype(F32)
    return high, middle, x - high - middle


class Ring:
    def __init__(self, axis, size, buf, send, recv):
        self.axis, self.size, self.buf, self.send, self.recv = axis, size, buf, send, recv
        self.me = lax.axis_index(axis)

    def last(self, way, part):
        return self.size // 2 if way == part else (self.size - 1) // 2

    def origin(self, way, step):
        if way == 0:
            return lax.rem(self.me - step + self.size, self.size)
        return lax.rem(self.me + step, self.size)

    def copy(self, way, part, step):
        slot = self.origin(way, step - 1)
        piece = self.buf.at[slot, pl.ds(part * CHUNK, CHUNK)]
        to = lax.rem(self.me + (1 if way == 0 else self.size - 1), self.size)
        return pltpu.make_async_remote_copy(
            src_ref=piece,
            dst_ref=piece,
            send_sem=self.send.at[way, part, step],
            recv_sem=self.recv.at[part, slot],
            device_id={self.axis: to},
            device_id_type=MESH,
        )

    def arrived(self, way, part, step):
        slot = self.origin(way, step)
        piece = self.buf.at[slot, pl.ds(part * CHUNK, CHUNK)]
        pltpu.make_async_remote_copy(
            src_ref=piece,
            dst_ref=piece,
            send_sem=self.send.at[way, part, step],
            recv_sem=self.recv.at[part, slot],
            device_id={self.axis: self.origin(way, 1)},
            device_id_type=MESH,
        ).wait_recv()

    def hop(self, step, part):
        for way in range(2):
            if 1 < step <= self.last(way, part) + 1:
                self.arrived(way, part, step - 1)
            if step <= self.last(way, part):
                self.copy(way, part, step).start()

    def drain(self):
        for part in range(2):
            for way in range(2):
                for step in range(1, self.last(way, part) + 1):
                    self.copy(way, part, step).wait_send()


def to_peer(src, dst, send, recv, axis, to):
    return pltpu.make_async_remote_copy(
        src_ref=src,
        dst_ref=dst,
        send_sem=send,
        recv_sem=recv,
        device_id={axis: to},
        device_id_type=MESH,
    )


def kernel(
    sizes,
    q_ref,
    k_ref,
    v_ref,
    f_ref,
    fgain_ref,
    r_ref,
    lk_ref,
    lv_ref,
    ll_ref,
    dl_ref,
    lgain_ref,
    wf_ref,
    wl_ref,
    out_ref,
    precv,
    both,
    wbuf,
    pairs,
    accs,
    tops,
    osend,
    okeep,
    hsend,
    hkeep,
    zkeep,
    esend,
    ekeep,
    psend,
    mixin,
    sums,
    ein,
    rin,
    eout,
    wout,
    grown,
    g_s,
    h_s,
    p_s,
    o_s,
    inside,
    ysend,
    yrecv,
    zsend,
    zrecv,
    wsend,
    wrecv,
    osem_send,
    osem_recv,
    hsem_send,
    hsem_recv,
    zsem_send,
    zsem_recv,
    esem_send,
    esem_recv,
    psem,
):
    n0, n1, nf = sizes
    z, y = lax.axis_index("sp_0"), lax.axis_index("sp_1")
    x, core = lax.axis_index("fs"), lax.axis_index("tp")
    lane128 = iota((TOK, 128), 1)

    low_lane = lane128 < HEAD
    ybuf, zbuf = both.at[0], both.at[1]

    def key_block(pair):
        keys = k_ref[...].astype(F32)
        if pair == 1:
            keys = pltpu.roll(keys, HEAD, 1)
        place = iota((128, TOK), 0)
        gates = jnp.zeros((128, TOK), F32)
        for member in range(2):
            line = -f_ref[2 * pair + member : 2 * pair + member + 1, :]
            for k, piece in enumerate(three_parts(line)):
                gates = jnp.where(place == HEAD + 3 * member + k, piece, gates)
        return jnp.where(low_lane, keys, jnp.transpose(gates)).astype(BF16)

    values_t = jnp.transpose(v_ref[...].astype(F32)).astype(BF16)
    queries = (q_ref[...].astype(F32) * 0.125).astype(BF16)
    ybuf[y, 0:TOK] = queries[:, :128]
    zbuf[z, 0:TOK] = queries[:, 128:]
    for pair, buf, slot in ((0, zbuf, z), (1, ybuf, y)):
        buf[slot, TOK : 2 * TOK] = key_block(pair)
        rows = slice(pair * HEAD, (pair + 1) * HEAD)
        buf[slot, 2 * TOK : 2 * TOK + HEAD] = values_t[rows, :128]
        buf[slot, 2 * TOK + HEAD : PACK] = values_t[rows, 128:]

    barrier = pltpu.get_barrier_semaphore()
    peers = [("sp_0", n0, z), ("sp_1", n1, y), ("fs", nf, x), ("tp", 2, core)]
    for axis, size, me in peers:
        for d in range(1, size):
            pl.semaphore_signal(
                barrier, inc=1, device_id={axis: lax.rem(me + d, size)}, device_id_type=MESH
            )
    pl.semaphore_wait(barrier, sum(size - 1 for _, size, _ in peers))

    rings = (Ring("sp_1", n1, ybuf, ysend, yrecv), Ring("sp_0", n0, zbuf, zsend, zrecv))

    def hop(step, part):
        for ring in rings:
            ring.hop(step, part)

    hop(1, 0)
    hop(1, 1)

    def weight_copies(d):
        to = lax.rem(x + d, nf)
        return [
            to_peer(
                ref,
                wbuf.at[x, pl.ds(part * WIDE, WIDE)],
                wsend.at[d, part],
                wrecv.at[part, x],
                "fs",
                to,
            )
            for part, ref in enumerate((wf_ref, wl_ref))
        ]

    row, col = iota((TOK, TOK), 0), iota((TOK, TOK), 1)
    same_span = (row // SPAN) == (col // SPAN)
    same_head = same_span
    strict = jnp.logical_and(same_span, row > col)
    lower = jnp.logical_and(same_span, row >= col)
    head_ones = same_head.astype(F32).astype(BF16)

    def head_sum(t):
        high = t.astype(BF16)
        rest = (t - high.astype(F32)).astype(BF16)
        return dot(high, head_ones) + dot(rest, head_ones)

    lkeys = lk_ref[...].astype(F32)
    unit = lkeys * lax.rsqrt(head_sum(lkeys * lkeys) + NORM_EPS)
    fall = -jnp.exp(dl_ref[...])
    lower_ones = lower.astype(F32).astype(BF16)
    inclusive = sum(dot(lower_ones, piece.astype(BF16)) for piece in three_parts(fall))
    grow = jnp.exp(inclusive)
    shrink = jnp.exp(-inclusive)
    grown[...] = grow
    ein[...] = (-unit * jnp.exp(inclusive - fall)).astype(BF16)
    rin[...] = r_ref[...].astype(F32) * grow
    eout[...] = unit * jax.nn.sigmoid(ll_ref[...].astype(F32)) * shrink
    wout[...] = lkeys * shrink

    for head in range(HEADS):
        in_head = (iota((TOK, WIDE), 1) // HEAD) == head

        def of_head(t):
            return jnp.where(in_head, t.astype(F32), 0.0).astype(BF16)

        e_in = ein[...]
        r_in = rin[...].astype(BF16)
        e_out = of_head(eout[...])
        w_out = of_head(wout[...])
        vals = of_head(lv_ref[...])
        mix_erase = jnp.where(strict, dot_t(e_in, e_out), 0.0)
        mix_write = jnp.where(strict, dot_t(e_in, w_out), 0.0).astype(BF16)
        read_erase = jnp.where(lower, dot_t(r_in, e_out), 0.0).astype(BF16)
        read_write = jnp.where(lower, dot_t(r_in, w_out), 0.0).astype(BF16)

        def level(size):
            odd = jnp.logical_and((row // size) % 2 == 1, (col // size) == (row // size) - 1)
            return jnp.where(odd, mix_erase, 0.0)

        inverse = jnp.where(row == col, 1.0, level(1))
        for size in (2, 4, 8, 16, 32):
            rounded = inverse.astype(BF16)
            step = dot(level(size).astype(BF16), rounded).astype(BF16)
            inverse = inverse + dot(rounded, step)
        inverse = inverse.astype(BF16)
        g_h = dot(inverse, of_head(e_in))
        h_h = dot(inverse, dot(mix_write, vals).astype(BF16))
        p_h = dot(read_erase, g_h.astype(BF16))
        o_h = dot(read_erase, h_h.astype(BF16)) + dot(read_write, vals)
        if head == 0:
            g_s[...], h_s[...], p_s[...], o_s[...] = g_h, h_h, rin[...] + p_h, o_h
        else:
            g_s[...] += g_h
            h_s[...] += h_h
            p_s[...] += p_h
            o_s[...] += o_h
        hop(2 + head // 2, head % 2)

    def compact(t):
        return t[0:64] + t[64:128] + t[128:192] + t[192:256]

    def expand(t):
        copies = t.shape[1] // HEAD
        wide = jnp.concatenate([t.astype(F32)] * copies, axis=0)
        return jnp.where(same_head[: wide.shape[0], : wide.shape[1]], wide, 0.0).astype(BF16)

    def after(earlier, decay, change, added):
        before_decay, before = earlier
        width, rows = before.shape[1], added.shape[0]
        diagonal = iota((64, width), 0) == iota((64, width), 1) % HEAD
        left = before + jnp.concatenate(
            [jnp.where(diagonal, before_decay, 0.0), jnp.zeros((rows, width), F32)], axis=0
        )
        grown_by = jnp.concatenate([jnp.zeros((64, width), F32), added], axis=0)
        return before_decay * decay, before * decay + dot(left.astype(BF16), change) + grown_by

    def decay_rows(decay):
        place = iota((16, decay.shape[1]), 0)
        tail = jnp.zeros((16, decay.shape[1]), F32)
        for k, piece in enumerate(three_parts(decay)):
            tail = jnp.where(place == k, piece, tail)
        return tail.astype(BF16)

    def get_map(t):
        tail = t[80:96].astype(F32)
        return tail[0:1] + tail[1:2] + tail[2:3], t[0:64], t[64:80].astype(F32)

    for span in range(TOK // SPAN):
        at = slice(span * SPAN, (span + 1) * SPAN)
        final = grown[at.stop - 1 : at.stop, :]
        e_f = (eout[at, :] * final).astype(BF16)
        w_f = (wout[at, :] * final).astype(BF16)
        change = jnp.where(same_head, t_dot(g_s[at, :].astype(BF16), e_f), 0.0)
        added = t_dot(h_s[at, :].astype(BF16), e_f) + t_dot(lv_ref[at, :], w_f)
        added = compact(jnp.where(same_head, added, 0.0))
        if span == 0:
            chain = (final, jnp.concatenate([compact(change), added], axis=0))
        else:
            p_span = p_s[at, :].astype(BF16)
            o_s[at, :] += dot_t(p_span, expand(chain[1][64:128]))
            p_s[at, :] = p_s[at, :] * chain[0] + dot_t(p_span, expand(chain[1][0:64]))
            chain = after(chain, final, change.astype(BF16), added)
    for u in range(n1):
        lanes, rows = slice((u // 4) * 128, (u // 4 + 1) * 128), 64 + 16 * (u % 4)
        hsend[u, 0:64] = chain[1][0:64, lanes].astype(BF16)
        hsend[u, 64:80] = chain[1][rows : rows + 16, lanes].astype(BF16)
        hsend[u, 80:96] = decay_rows(chain[0][:, lanes])
    hkeep[y] = hsend[y]

    def handler_copy(d):
        to = lax.rem(y + d, n1)
        return to_peer(
            hsend.at[to], hkeep.at[y], hsem_send.at[d], hsem_recv.at[y], "sp_1", to
        )

    def entry_copy(d):
        to = lax.rem(y + d, n1)
        return to_peer(
            esend.at[to], ekeep.at[y], esem_send.at[d], esem_recv.at[y], "sp_1", to
        )

    def column_copy(d):
        to = lax.rem(z + d, n0)
        return to_peer(zkeep.at[z], zkeep.at[z], zsem_send.at[d], zsem_recv.at[z], "sp_0", to)

    def from_row(keep, send, recv):
        def one(d, _):
            slot = lax.rem(y + d, n1)
            to_peer(keep.at[slot], keep.at[slot], send.at[d], recv.at[slot], "sp_1", slot).wait_recv()
            return 0

        lax.fori_loop(1, n1, one, 0)

    def states_row():
        from_row(hkeep, hsem_send, hsem_recv)
        decay, change, added = get_map(hkeep[0])
        first = (decay, jnp.concatenate([change.astype(F32), added], axis=0))

        def follow(k, so_far):
            inside[k, 0:80] = so_far[1]
            inside[k, 80:88] = jnp.broadcast_to(so_far[0], (8, 128))
            decay, change, added = get_map(hkeep[k])
            return after(so_far, decay, expand(change), added)

        decay, whole = lax.fori_loop(1, n1, follow, first)
        zkeep[z, 0:80] = whole.astype(BF16)
        zkeep[z, 80:96] = decay_rows(decay)

        def send(d, _):
            column_copy(d).start()
            return 0

        lax.fori_loop(1, n0 - z, send, 0)

    def states_column():
        def arrived(slot, _):
            to_peer(
                zkeep.at[slot], zkeep.at[slot], zsem_send.at[0], zsem_recv.at[slot], "sp_0", slot
            ).wait_recv()
            return 0

        lax.fori_loop(0, z, arrived, 0)

        def enter(k, state):
            decay, change, added = get_map(zkeep[k])
            return state * decay + dot(state.astype(BF16), expand(change)) + added

        entry = lax.fori_loop(0, z, enter, jnp.zeros((16, 128), F32))
        esend[0] = entry.astype(BF16)
        for k in range(1, n1):
            here = inside[k]
            moved = entry * here[80:81] + dot(entry.astype(BF16), expand(here[0:64]))
            esend[k] = (moved + here[64:80]).astype(BF16)
        ekeep[y] = esend[y]
        for d in range(1, n1):
            entry_copy(d).start()

    hop(4, 0)
    for d in range(1, n1):
        handler_copy(d).start()
    for d in range(1, nf):
        for copy in weight_copies(d):
            copy.start()
    wbuf[x, 0:WIDE] = wf_ref[...]
    wbuf[x, WIDE : 2 * WIDE] = wl_ref[...]

    def query_pair(raw):
        wide = raw.astype(F32)
        ones = [
            jnp.where(
                jnp.logical_and(lane128 >= HEAD + 3 * m, lane128 < HEAD + 3 * m + 3), 1.0, 0.0
            )
            for m in range(2)
        ]
        first = jnp.where(low_lane, wide, ones[0])
        second = jnp.where(low_lane, pltpu.roll(wide, HEAD, 1), ones[1])
        return jnp.concatenate([first, second], axis=0).astype(BF16)

    def scores_of(q_pair, buf, slots):
        keys = [buf[slot, TOK : 2 * TOK] for slot in slots]
        return dot_t(jnp.concatenate(keys, axis=0) if len(keys) > 1 else keys[0], q_pair)

    def values_of(buf, slots):
        return jnp.concatenate(
            [
                buf[slot, 2 * TOK + part * HEAD : 2 * TOK + (part + 1) * HEAD]
                for slot in slots
                for part in range(2)
            ],
            axis=1,
        )

    def absorb(scores, vals, carry):
        top, total, acc = carry
        new_top = jnp.maximum(top, jnp.max(scores, axis=0, keepdims=True))
        scale = jnp.exp(top - new_top)
        weights = jnp.exp(scores - new_top)
        total = total * scale + jnp.sum(weights, axis=0, keepdims=True)
        return new_top, total, acc * scale + dot(vals, weights.astype(BF16))

    def load(group, block):
        return tops[group, block, 0:1], tops[group, block, 1:2], accs[group, block]

    def save(group, block, carry):
        tops[group, block, 0:1], tops[group, block, 1:2], accs[group, block] = carry

    def put(ref, group, slot, carry):
        top, total, acc = carry
        place = iota((16, TOK), 0)
        tail = jnp.zeros((16, TOK), F32)
        for which, line in enumerate((top, total)):
            for k, piece in enumerate(three_parts(line)):
                for member in range(2):
                    part = piece[:, member * TOK : (member + 1) * TOK]
                    tail = jnp.where(place == 6 * which + 3 * member + k, part, tail)
        acc = acc.astype(BF16)
        ref[group, slot, 0:HEAD] = acc[:, :TOK]
        ref[group, slot, HEAD : 2 * HEAD] = acc[:, TOK:]
        ref[group, slot, 2 * HEAD : 2 * HEAD + 16] = tail.astype(BF16)

    tops[:, :, 0:1] = jnp.full((2, tops.shape[1], 1, 2 * TOK), LOW, F32)
    tops[:, :, 1:2] = jnp.zeros((2, tops.shape[1], 1, 2 * TOK), F32)
    accs[...] = jnp.zeros(accs.shape, F32)

    def given(group, to, giver):
        seen = jnp.logical_or(z > 0, giver < to)
        return jnp.where(group == 0, seen, giver < to)

    for group, size, me in ((0, n1, y), (1, n0, z)):

        def no_keys(d, _):
            slot = lax.rem(me + d, size)

            @pl.when(jnp.logical_not(given(group, me, slot)))
            def _():
                place = iota((16, TOK), 0)
                low = jnp.where(jnp.logical_or(place == 0, place == 3), LOW, 0.0)
                okeep[group, slot, 0 : 2 * HEAD] = jnp.zeros((2 * HEAD, TOK), BF16)
                okeep[group, slot, 2 * HEAD : 2 * HEAD + 16] = low.astype(BF16)

            return 0

        lax.fori_loop(1, size, no_keys, 0)

    def gives(group, d):
        me, size = jnp.where(group == 0, y, z), jnp.where(group == 0, n1, n0)
        return jnp.logical_and(d < size, given(group, lax.rem(me + d, size), me))

    reach0 = reach1 = min(1, (n0 - 1) // 2, (n1 - 1) // 2)
    row_of, column_of = ("sp_1", n1, y, reach1), ("sp_0", n0, z, reach0)

    def make_pairs(group, first, count):
        axis, size, me, reach = (row_of, column_of)[group]

        def one(d, _):
            block = lax.rem(me + (first % size) + d, size)
            pairs[group, block] = query_pair(both[group, block, 0:TOK])
            return 0

        lax.fori_loop(0, count, one, 0)

    def near(radius):
        side = 2 * radius

        def one(k, _):
            picked = []
            for down, right in ((0, k), (k, side), (side, side - k), (side - k, 0)):
                i = lax.rem(z + down + (n0 - radius), n0)
                j = lax.rem(y + right + (n1 - radius), n1)
                first = jnp.logical_or(i < z, jnp.logical_and(i == z, y < j))
                group = jnp.where(first, 0, 1)
                block, slot = jnp.where(first, j, i), jnp.where(first, i, j)
                buf = both.at[1 - group]
                picked.append((group, block, buf, slot, scores_of(pairs[group, block], buf, [slot])))
            for group, block, buf, slot, scores in picked:
                save(group, block, absorb(scores, values_of(buf, [slot]), load(group, block)))
            return 0

        lax.fori_loop(0, side, one, 0)

    make_pairs(0, -reach1, 2 * reach1 + 1)
    make_pairs(1, -reach0, 2 * reach0 + 1)
    for group, me, slot in ((0, y, z), (1, z, y)):
        carry = load(group, me)
        buf = both.at[1 - group]
        allowed = iota((TOK, 2 * TOK), 0) <= iota((TOK, 2 * TOK), 1) % TOK
        scores = jnp.where(allowed, scores_of(pairs[group, me], buf, [slot]), LOW)
        save(group, me, absorb(scores, values_of(buf, [slot]), carry))
    hop(4, 1)
    if reach0 > 0:
        near(1)
    hop(5, 0)
    hop(5, 1)
    make_pairs(0, reach1 + 1, n1 - 2 * reach1 - 1)
    make_pairs(1, reach0 + 1, n0 - 2 * reach0 - 1)

    def rest(group, d):
        rows = group == 0
        block = lax.rem(jnp.where(rows, y, z) + d, jnp.where(rows, n1, n0))
        mine, count = jnp.where(rows, z, y), jnp.where(rows, n0, n1)
        is_near = jnp.logical_or(d <= reach0, d >= jnp.where(rows, n1, n0) - reach0)
        start_a = jnp.maximum(jnp.where(is_near, reach0 + 1, 1), n0 - z)
        end_a = jnp.where(is_near, n0 - reach0, n0 + jnp.where(y < block, 1, 0))
        start_b = jnp.where(is_near, reach1 + 1, 0)
        start_b = jnp.where(d == 0, jnp.maximum(start_b, n1 - y), start_b)
        end_b = jnp.where(is_near, n1 - reach1, n1)
        end_b = jnp.where(jnp.logical_and(d > 0, block < z), start_b, end_b)
        start = jnp.where(rows, start_a, start_b)
        length = jnp.maximum(jnp.where(rows, end_a, end_b) - start, 0)
        buf = both.at[1 - group]

        def step(size):
            def one(at, carry):
                slots = [lax.rem(mine + at + k, count) for k in range(size)]
                scores = scores_of(pairs[group, block], buf, slots)
                return absorb(scores, values_of(buf, slots), carry)

            return one

        eights = length // 8
        carry = lax.fori_loop(
            0, eights, lambda k, carry: step(8)(start + 8 * k, carry), load(group, block)
        )
        at = start + 8 * eights
        fours = (length - 8 * eights) // 4
        carry = lax.fori_loop(0, fours, lambda k, carry: step(4)(at + 4 * k, carry), carry)
        at = at + 4 * fours
        twos = (start + length - at) // 2
        carry = lax.fori_loop(0, twos, lambda k, carry: step(2)(at + 2 * k, carry), carry)
        at = at + 2 * twos
        return lax.fori_loop(
            0, start + length - at, lambda k, carry: step(1)(at + k, carry), carry
        )

    def output_copy(group, d):
        rows = group == 0
        me = jnp.where(rows, y, z)
        to = lax.rem(me + d, jnp.where(rows, n1, n0))
        return pltpu.make_async_remote_copy(
            src_ref=osend.at[group, d],
            dst_ref=okeep.at[group, me],
            send_sem=osem_send.at[group, d],
            recv_sem=osem_recv.at[group, me],
            device_id={"sp_0": jnp.where(rows, z, to), "sp_1": jnp.where(rows, to, y)},
            device_id_type=MESH,
        )

    longest = max(n0, n1)
    row_turn, column_turn = 2 % (2 * longest - 2), min(7, 2 * longest - 3)

    def finish(t, _):
        group, turn = t % 2, t // 2
        d = longest // 2 + jnp.where(turn % 2 == 1, -((turn + 1) // 2), turn // 2)

        @pl.when(t == row_turn)
        def _():
            states_row()

        @pl.when(t == column_turn)
        def _():
            states_column()

        @pl.when(gives(group, d))
        def _():
            put(osend, group, d, rest(group, d))
            output_copy(group, d).start()

        return 0

    lax.fori_loop(0, 2 * (longest - 1), finish, 0)

    def own(group, _):
        put(okeep, group, jnp.where(group == 0, y, z), rest(group, 0))
        return 0

    lax.fori_loop(0, 2, own, 0)

    from_row(ekeep, esem_send, esem_recv)
    entry = jnp.concatenate(
        [
            jnp.concatenate([ekeep[4 * tile_of + k] for k in range(4)], axis=0)
            for tile_of in range(2)
        ],
        axis=1,
    )
    read = o_s[...] + dot_t(p_s[...].astype(BF16), expand(entry))
    centred = read - head_sum(read) * (1.0 / HEAD)
    normed = centred * lax.rsqrt(head_sum(centred * centred) * (1.0 / HEAD) + HEAD * 1e-05)
    mixin[:, WIDE:] = (normed * lgain_ref[...]).astype(BF16)

    for d in range(1, nf):
        slot = lax.rem(x + d, nf)
        for part in range(2):
            piece = wbuf.at[slot, pl.ds(part * WIDE, WIDE)]
            to_peer(piece, piece, wsend.at[d, part], wrecv.at[part, slot], "fs", slot).wait_recv()
    columns = wf_ref.shape[1]
    slices = [slice(slot * columns, (slot + 1) * columns) for slot in range(nf)]
    lin_out = mixin[:, WIDE:]
    for slot, at in enumerate(slices):
        sums[:, at] = dot(lin_out, wbuf[slot, WIDE : 2 * WIDE])

    def joined(group):
        axis, size, me, reach = (row_of, column_of)[group]

        def wait(d, _):
            slot = lax.rem(me + d, size)
            piece = okeep.at[group, slot]

            @pl.when(given(group, me, slot))
            def _():
                to_peer(
                    piece, piece, osem_send.at[group, d], osem_recv.at[group, slot], axis, slot
                ).wait_recv()

            return 0

        lax.fori_loop(1, size, wait, 0)
        lines = []
        for slot in range(size):
            tail = okeep[group, slot, 2 * HEAD : 2 * HEAD + 16].astype(F32)
            lines.append([tail[3 * k : 3 * k + 1] + tail[3 * k + 1 : 3 * k + 2] + tail[3 * k + 2 : 3 * k + 3] for k in range(4)])
        heads = []
        for member in range(2):
            top = functools.reduce(jnp.maximum, [line[member] for line in lines])
            total, acc = 0.0, 0.0
            for slot in range(size):
                scale = jnp.exp(lines[slot][member] - top)
                total = total + scale * lines[slot][2 + member]
                part = okeep[group, slot, member * HEAD : (member + 1) * HEAD]
                acc = acc + scale * part.astype(F32)
            acc = acc * (1.0 / total)
            square = jnp.sum(acc * acc, axis=0, keepdims=True) * (1.0 / HEAD)
            heads.append(acc * lax.rsqrt(square + NORM_EPS))
        return jnp.concatenate(heads, axis=0)

    mixed = jnp.concatenate([joined(0), joined(1)], axis=0)
    mixin[:, :WIDE] = (jnp.transpose(mixed) * fgain_ref[...]).astype(BF16)

    half = TOK // 2
    partner = 1 - core
    theirs = pl.ds(pl.multiple_of(partner * half, half), half)
    mine = pl.ds(pl.multiple_of(core * half, half), half)
    for slot, at in enumerate(slices):
        added = dot(mixin[theirs, :WIDE], wbuf[slot, 0:WIDE])
        psend[:, at] = (sums[theirs, at] + added).astype(BF16)
    swap = to_peer(psend, precv, psem.at[0], psem.at[1], "tp", partner)
    swap.start()
    for slot, at in enumerate(slices):
        added = dot(mixin[mine, :WIDE], wbuf[slot, 0:WIDE])
        out_ref[:, at] = (sums[mine, at] + added).astype(BF16)
    swap.wait()

    for ring in rings:
        ring.drain()
    for d in range(1, nf):
        for copy in weight_copies(d):
            copy.wait_send()
    for d in range(1, n1):
        handler_copy(d).wait_send()
        entry_copy(d).wait_send()

    def column_left(d, _):
        column_copy(d).wait_send()
        return 0

    lax.fori_loop(1, n0 - z, column_left, 0)
    for group, size in ((0, n1), (1, n0)):

        def output_left(d, _):
            @pl.when(gives(group, d))
            def _():
                output_copy(group, d).wait_send()

            return 0

        lax.fori_loop(1, size, output_left, 0)


def solution(mesh):
    nf, n_tp = mesh.shape["fs"], mesh.shape["tp"]
    n0 = 8 if mesh.shape["sp"] == 64 else mesh.shape["sp"] // 2
    n1 = mesh.shape["sp"] // n0
    finer = Mesh(mesh.devices.reshape(n0, n1, nf, n_tp), ("sp_0", "sp_1", "fs", "tp"))

    def shards(q, k, v, f, fgain, r, lk, lv, ll, dl, lgain, wf, wl):
        width = wf.shape[1] * nf
        vm = pl.BlockSpec(memory_space=pltpu.VMEM)
        dma = pltpu.SemaphoreType.DMA
        wide32 = pltpu.VMEM((TOK, WIDE), F32)
        most = max(n0, n1)
        part = (2, most, 2 * HEAD + 16, TOK)
        own, partner = pl.pallas_call(
            functools.partial(kernel, (n0, n1, nf)),
            out_shape=[jax.ShapeDtypeStruct((TOK // 2, width), BF16)] * 2,
            in_specs=[vm] * 13,
            out_specs=[vm, vm],
            scratch_shapes=[
                pltpu.VMEM((2, most, PACK, 128), BF16),
                pltpu.VMEM((nf, 2 * WIDE, wf.shape[1]), BF16),
                pltpu.VMEM((2, most, 2 * TOK, 128), BF16),
                pltpu.VMEM((2, most, HEAD, 2 * TOK), F32),
                pltpu.VMEM((2, most, 8, 2 * TOK), F32),
                pltpu.VMEM(part, BF16),
                pltpu.VMEM(part, BF16),
                pltpu.VMEM((n1, 96, 128), BF16),
                pltpu.VMEM((n1, 96, 128), BF16),
                pltpu.VMEM((n0, 96, 128), BF16),
                pltpu.VMEM((n1, 16, 128), BF16),
                pltpu.VMEM((n1, 16, 128), BF16),
                pltpu.VMEM((TOK // 2, width), BF16),
                pltpu.VMEM((TOK, 2 * WIDE), BF16),
                pltpu.VMEM((TOK, width), F32),
                pltpu.VMEM((TOK, WIDE), BF16),
                wide32,
                wide32,
                wide32,
                wide32,
                wide32,
                wide32,
                wide32,
                wide32,
                pltpu.VMEM((n1, 88, 128), F32),
                dma((2, 2, n1 // 2 + 1)),
                dma((2, n1)),
                dma((2, 2, n0 // 2 + 1)),
                dma((2, n0)),
                dma((nf, 2)),
                dma((2, nf)),
                dma((2, most)),
                dma((2, most)),
                dma((n1,)),
                dma((n1,)),
                dma((n0,)),
                dma((n0,)),
                dma((n1,)),
                dma((n1,)),
                dma((2,)),
            ],
            compiler_params=pltpu.CompilerParams(
                collective_id=0, has_side_effects=True, vmem_limit_bytes=60 * 1024 * 1024
            ),
        )(
            q[0], k[0], v[0], f[0].T, fgain[None], r[0], lk[0], lv[0], ll[0], dl[0], lgain[None], wf, wl
        )
        return (own.astype(F32) + partner.astype(F32)).astype(BF16)[None]

    heads = P("fs", SP, "tp")
    gains, weights = P("tp"), P("tp", "fs")
    placed = (heads,) * 4 + (gains,) + (heads,) * 5 + (gains, weights, weights)
    return jax.shard_map(
        shards, mesh=finer, in_specs=placed, out_specs=P("fs", SP_TP, None), check_vma=False
    )
```
